32 devices in a mesh: grp: 2 (over y), row: 4 (over z), col: 4 (over x, core).
Axes of the slice: x: 2, y: 2, z: 4, core: 2. Of those that a mesh axis runs over, the one named last changes fastest.
Arguments:
- tokens: bfloat16 [2048, 2048], P(('grp', 'row')), parts along dimension 0, may hold values from -6 to 6
- w_value: bfloat16 [2048, 2048], P(None, 'col'), may hold values from -0.125 to 0.125
- w_gate_a: bfloat16 [2048, 2048], P(None, 'col'), may hold values from -0.125 to 0.125
- w_gate_b: bfloat16 [2048, 2048], P(None, 'col'), may hold values from -0.125 to 0.125
- short_taps: bfloat16 [3, 3, 2048], replicated, may hold values from -3.5 to 3.5
- pos_weight: float32 [33, 64], replicated, may hold values from -3 to 3
- pos_bias: float32 [64], replicated, may hold values from -3 to 3
- sine_freq: float32 [2, 64], replicated, may hold values from 1.2 to 2
- hid_weight: float32 [64, 64], replicated, may hold values from -1.5 to 1.5
- hid_bias: float32 [64], replicated, may hold values from -3 to 3
- filter_out: float32 [64, 2, 2, 2048], P(None, None, None, 'col'), may hold values from -0.046875 to 0.046875
- filter_bias: float32 [2, 2048], replicated, may hold values from -3 to 3
- lag_decay: float32 [2048], replicated, may hold values from 1 to 35, as said below
Outputs:
- mixed: bfloat16 [2048, 2048], P(('grp', 'row'), 'col'), parts along dimension 0
The draws below stay inside these ranges and needn't reach their ends.
There are 2 independent parts, one for each index of `grp`. The reference program is written for one: setup_inputs(seed, part) draws one part's arguments, and reference() takes and returns one part's arrays. A program takes and returns all parts, laid end to end along the dimension named above; an argument that names none is the same for every part. Nothing has to cross between parts.
Inputs may be any that keep to these rules, and one draw needn't show every extreme that they name: `lag_decay`: each channel's envelope decay is positive.
All inputs are finite; a program needn't handle non-finite values.
Results may differ from the reference program's by a relative error of at most 0.0081.
Values may be sent and summed in bfloat16 or wider, within the bound.
A program may use at most 64 MiB of HBM per device.

```python
import math
import jax
import jax.numpy as jnp
from jax import lax

D = 2048
HID = 64
PE = 33
SEQ = 1024


def draw_lag_decay(key, part):
    pick_key = jax.random.fold_in(key, 11)
    slow_key = jax.random.fold_in(key, 12)
    fast_key = jax.random.fold_in(key, 13)
    slow_rates = jnp.exp(jax.random.uniform(slow_key, (D,), jnp.float32, 0.0, math.log(2.3)))
    fast_low = max(SEQ / 100.0, 3.0)
    fast_high = max(SEQ / 30.0, 6.0)
    fast_rates = jnp.exp(jax.random.uniform(fast_key, (D,), jnp.float32, math.log(fast_low), math.log(fast_high)))
    fast_share = 0.5
    chosen = jax.random.bernoulli(pick_key, fast_share, (D,))
    return jnp.where(chosen, fast_rates, slow_rates).astype(jnp.float32)


def shard_levels(own_key, dims, split, smallest, top_value):
    def one(axis_at, parts):
        heights = jax.random.uniform(jax.random.fold_in(jax.random.fold_in(own_key, 6), axis_at), (parts,), jnp.float32, smallest / len(split), top_value / len(split))
        return jnp.repeat(jnp.exp(heights), dims[axis_at] // parts).reshape((-1,) + (1,) * (len(dims) - axis_at - 1))

    level = one(*split[0])
    for cut in split[1:]:
        level = level * one(*cut)
    return level


def centred(key, shape, spread, most, cuts=(), kind=jnp.bfloat16):
    loudness = shard_levels(key, shape, cuts, -0.22, 0.18) if cuts else 1.0
    entries = jax.random.normal(key, shape, jnp.float32) * spread * loudness
    return jnp.minimum(jnp.maximum(entries, -most), most).astype(kind)


def setup_inputs(seed: int = 0, part: int = 0) -> dict:
    key_of = jax.random.split(jax.random.key(seed), 14)
    part_keys = jax.random.split(jax.random.fold_in(key_of[13], part), 14)
    tokens = centred(part_keys[0], (SEQ, D), 1.0, 6.0, ((0, 4),))
    w_value = centred(key_of[1], (D, D), D ** -0.5, 0.125, ((1, 4),))
    w_gate_a = centred(key_of[2], (D, D), D ** -0.5, 0.125, ((1, 4),))
    w_gate_b = centred(key_of[3], (D, D), D ** -0.5, 0.125, ((1, 4),))
    short_taps = centred(key_of[4], (3, 3, D), 3 ** -0.5, 3.5)
    pos_weight = centred(key_of[5], (PE, HID), 1.0, 3.0, (), jnp.float32)
    pos_bias = centred(key_of[6], (HID,), 0.5, 3.0, (), jnp.float32)
    sine_freq = jnp.clip(jax.random.uniform(key_of[7], (2, HID), jnp.float32, 1.2, 2.0), 1.2, 2.0)
    hid_weight = centred(key_of[8], (HID, HID), 0.5, 1.5, (), jnp.float32)
    hid_bias = centred(key_of[9], (HID,), 0.5, 3.0, (), jnp.float32)
    filter_out = centred(key_of[10], (HID, 2, 2, D), (HID * SEQ // 4) ** -0.5, 0.046875, ((3, 4),), jnp.float32)
    filter_bias = centred(key_of[11], (2, D), 0.5, 3.0, (), jnp.float32)
    lag_decay = draw_lag_decay(jax.random.fold_in(key_of[13], 71), part)
    return dict(tokens=tokens, w_value=w_value, w_gate_a=w_gate_a, w_gate_b=w_gate_b, short_taps=short_taps, pos_weight=pos_weight, pos_bias=pos_bias, sine_freq=sine_freq, hid_weight=hid_weight, hid_bias=hid_bias, filter_out=filter_out, filter_bias=filter_bias, lag_decay=lag_decay)


WINDOW_SHIFT = 0.05


def positional_features(length):
    positions = jnp.arange(length, dtype=jnp.float32)
    scaled_time = positions / max(length - 1, 1)
    band_count = (PE - 1) // 2
    frequencies = jnp.linspace(1e-4, band_count - 1, band_count, dtype=jnp.float32)
    angles = ((2.0 * math.pi / length) * positions)[:, None] * frequencies[None, :]
    features = jnp.concatenate([scaled_time[:, None], jnp.cos(angles), -jnp.sin(angles)], axis=1)
    return scaled_time, features


def short_conv(projected, tap_weights):
    widened = jnp.pad(projected.astype(jnp.float32), ((1, 1), (0, 0)))
    tap_values = tap_weights.astype(jnp.float32)
    summed = widened[:-2] * tap_values[0] + widened[1:-1] * tap_values[1] + widened[2:] * tap_values[2]
    return summed.astype(jnp.bfloat16)


def long_conv(signal, forward_part, backward_part, bias_row):
    length = signal.shape[0]
    kernel = jnp.concatenate([forward_part, jnp.zeros_like(forward_part[:1]), backward_part[:0:-1]], axis=0)
    spectrum = jnp.fft.rfft(kernel, axis=0)
    transformed = jnp.fft.rfft(signal, n=2 * length, axis=0)
    result = jnp.fft.irfft(transformed * spectrum, n=2 * length, axis=0)[:length]
    return result + signal * bias_row


def reference(tokens, w_value, w_gate_a, w_gate_b, short_taps, pos_weight, pos_bias, sine_freq, hid_weight, hid_bias, filter_out, filter_bias, lag_decay):
    projections = [jnp.dot(tokens, weight_matrix, preferred_element_type=jnp.float32).astype(jnp.bfloat16) for weight_matrix in (w_value, w_gate_a, w_gate_b)]
    value_seq = short_conv(projections[0], short_taps[0])
    gate_a_seq = short_conv(projections[1], short_taps[1])
    gate_b_seq = short_conv(projections[2], short_taps[2])
    highest = lax.Precision.HIGHEST
    scaled_time, features = positional_features(SEQ)
    hidden_a = jnp.sin(sine_freq[0] * (jnp.dot(features, pos_weight, precision=highest) + pos_bias))
    hidden_b = jnp.sin(sine_freq[1] * (jnp.dot(hidden_a, hid_weight, precision=highest) + hid_bias))
    envelope = jnp.exp(-scaled_time[:, None] * lag_decay[None, :]) + WINDOW_SHIFT

    def order_filters(order_index):
        raw_filters = jnp.dot(hidden_b, filter_out[:, order_index].reshape(HID, 2 * D), precision=highest)
        raw_filters = raw_filters.reshape(SEQ, 2, D)
        return raw_filters[:, 0] * envelope, raw_filters[:, 1] * envelope

    forward_a, backward_a = order_filters(0)
    first_conv = long_conv(value_seq.astype(jnp.float32), forward_a, backward_a, filter_bias[0])
    gated = gate_a_seq.astype(jnp.float32) * first_conv
    forward_b, backward_b = order_filters(1)
    second_conv = long_conv(gated, forward_b, backward_b, filter_bias[1])
    return (gate_b_seq.astype(jnp.float32) * second_conv).astype(jnp.bfloat16)
```

```python
import functools
import math

import jax
import jax.numpy as jnp
import numpy as np
from jax import lax
from jax.experimental import pallas as pl
from jax.experimental.pallas import tpu as pltpu
from jax.sharding import PartitionSpec as P

WINDOW_SHIFT = 0.05
LEAF = 128
CHUNK = 16
MESH = pl.DeviceIdType.MESH
F32 = jnp.float32
BF16 = jnp.bfloat16


def leaf_angles(theta, count):
    if count == 1:
        return [theta]
    half = theta / 2
    return leaf_angles(half, count // 2) + leaf_angles(half + math.pi, count // 2)


def split_np(values):
    high = values.astype(jnp.bfloat16)
    low = (values - high.astype(np.float64)).astype(jnp.bfloat16)
    return high, low


@functools.lru_cache(maxsize=None)
def tables(seq, lanes, features, hidden):
    k = np.arange(LEAF)
    angle = 2 * np.pi / LEAF * ((k[:, None] * k[None, :]) % LEAF)
    cos, sin = np.cos(angle), np.sin(angle)
    forward = np.block([[cos, -sin], [sin, cos]])
    inverse = np.block([[cos, sin], [-sin, cos]]) / seq
    fcat = np.concatenate(split_np(forward), axis=0)
    gcat = np.concatenate(split_np(inverse), axis=0)
    thetas = np.array(leaf_angles(math.pi / 2, seq // LEAF))
    twist = (thetas[:, None] * k[None, :] / LEAF).reshape(-1)
    twist = np.stack([np.cos(twist), np.sin(twist)]).astype(np.float32)
    twist = np.ascontiguousarray(np.broadcast_to(twist[:, :, None], (2, seq, lanes)))
    bands = (features - 1) // 2
    freq = np.linspace(0.0001, bands - 1, bands, dtype=np.float32)

    def feats(positions):
        positions = positions.astype(np.float32)
        scaled = positions / np.float32(max(seq - 1, 1))
        ang = (np.float32(2.0 * math.pi / seq) * positions)[:, None] * freq[None, :]
        ang = ang.astype(np.float64)
        return np.concatenate([scaled[:, None], np.cos(ang), -np.sin(ang)], axis=1)

    both = np.zeros((seq, 2 * hidden))
    both[:, :features] = feats(np.arange(seq))
    both[:, hidden : hidden + features] = feats(seq - np.arange(seq))
    fhi, flo = split_np(both)
    return fcat, gcat, twist, fhi, flo


def split(x):
    high = x.astype(BF16)
    return high, (x - high.astype(F32)).astype(BF16)


def dot(a, b):
    return jnp.dot(a, b, preferred_element_type=F32)


def dot3(a, b):
    return dot(a[0], b[0]) + dot(a[1], b[0]) + dot(a[0], b[1])


PI_A = 3.140625
PI_B = float(np.float32(math.pi - 3.140625))
PI_C = float(math.pi - 3.140625 - np.float32(math.pi - 3.140625))


def sine(x):
    k = jnp.floor(x * (1.0 / math.pi) + 0.5)
    r = x - k * PI_A
    r = r - k * PI_B
    r = r - k * PI_C
    parity = k - 2.0 * jnp.floor(k * 0.5)
    s = r * r
    p = -1.0 / 39916800.0
    for c in (1.0 / 362880.0, -1.0 / 5040.0, 1.0 / 120.0, -1.0 / 6.0):
        p = p * s + c
    return (r + r * s * p) * (1.0 - 2.0 * parity)


def split_tree(blocks, theta):
    if len(blocks) == 1:
        return blocks
    half = len(blocks) // 2
    wr, wi = math.cos(theta / 2), math.sin(theta / 2)
    up, down = [], []
    for (ar, ai), (br, bi) in zip(blocks[:half], blocks[half:]):
        if bi is None:
            tr, ti = br * wr, br * wi
            up.append((ar + tr, ti))
            down.append((ar - tr, -ti))
        else:
            tr, ti = br * wr - bi * wi, br * wi + bi * wr
            up.append((ar + tr, ai + ti))
            down.append((ar - tr, ai - ti))
    return split_tree(up, theta / 2) + split_tree(down, theta / 2 + math.pi)


def join_tree(leaves, theta, top):
    if len(leaves) == 1:
        return leaves
    half = len(leaves) // 2
    up = join_tree(leaves[:half], theta / 2, False)
    down = join_tree(leaves[half:], theta / 2 + math.pi, False)
    wr, wi = math.cos(theta / 2), math.sin(theta / 2)
    first, second = [], []
    for (pr, pi), (qr, qi) in zip(up, down):
        dr, di = pr - qr, pi - qi
        if top:
            first.append(pr + qr)
            second.append(dr * wr + di * wi)
        else:
            first.append((pr + qr, pi + qi))
            second.append((dr * wr + di * wi, di * wr - dr * wi))
    return first + second


def kernel(
    sizes,
    tok_h, wv_h, wa_h, wb_h, fcat_h, gcat_h, twist_h, fhi_h, flo_h,
    wf_h, own_taps_h, gate_taps_h, pw_h, pb_h, sf_h, hw_h, hb_h, fb_h, ld_h,
    out_ref,
    own_taps, gate_taps, pw, pb, sf, hw, hb, fb, ld,
    tok, wva, wb, fcat, gcat, twist, fhi, flo,
    wf, sbuf, rbuf, gb, halo, pad, xs, gs, gpad, gbs,
    pwb, hwb, wfb, kre, kim, xhi, xlo, spec, ybuf, s2, r2,
    in_sem, send_sem, recv_sem, halo_send, halo_recv, back_send, back_recv,
):
    R, T, N, C, S, HID, PE = sizes
    L = N // LEAF
    row = lax.axis_index("row")
    col = lax.axis_index("col")
    aligned = C % 128 == 0
    if aligned:
        own_at = pl.ds(pl.multiple_of(col * S + row * C, 128), C)
        share_at = pl.ds(pl.multiple_of(col * S, 128), S)
    else:
        own_at, share_at = slice(0, C), slice(0, S)

    half = R // 2
    H = S // 2
    far = 1 - row // half
    order = [far, 1 - far]

    def load(i, src, dst):
        copy = pltpu.make_async_copy(src, dst, in_sem.at[i])
        copy.start()
        return copy

    def load_half(i, src, which, k):
        lanes = pl.ds(pl.multiple_of(order[k] * H, H), H)
        return load(i, src.at[:, lanes], wva.at[k, :, which * H : (which + 1) * H])

    ld_tok = load(0, tok_h, tok)
    ld_half = [
        [load_half(2 * k + which + 1, src, which, k) for which, src in enumerate((wv_h, wa_h))]
        for k in range(2)
    ]

    barrier = pltpu.get_barrier_semaphore()
    peers = [lax.rem(row + d, R) for d in range(R)]
    sources = [lax.rem(row + R - d, R) for d in range(R)]
    for d in range(1, R):
        pl.semaphore_signal(barrier, inc=1, device_id={"row": peers[d]}, device_id_type=MESH)

    def out_copy(which, target, slot):
        return pltpu.make_async_remote_copy(
            src_ref=sbuf.at[which, target], dst_ref=rbuf.at[which, row],
            send_sem=send_sem.at[which, slot], recv_sem=recv_sem.at[which, row],
            device_id={"row": target}, device_id_type=MESH)

    def in_copy(which, d):
        return pltpu.make_async_remote_copy(
            src_ref=sbuf.at[which, peers[d]], dst_ref=rbuf.at[which, sources[d]],
            send_sem=send_sem.at[which, d], recv_sem=recv_sem.at[which, sources[d]],
            device_id={"row": peers[d]}, device_id_type=MESH)

    def halo_copy(side):
        src = gb.at[pl.ds(T - CHUNK, CHUNK)] if side == 0 else gb.at[pl.ds(0, CHUNK)]
        target = peers[1] if side == 0 else peers[R - 1]
        return pltpu.make_async_remote_copy(
            src_ref=src, dst_ref=halo.at[side],
            send_sem=halo_send.at[side], recv_sem=halo_recv.at[side],
            device_id={"row": target}, device_id_type=MESH)

    def back_out(d):
        return pltpu.make_async_remote_copy(
            src_ref=s2.at[peers[d]], dst_ref=r2.at[row],
            send_sem=back_send.at[d], recv_sem=back_recv.at[d],
            device_id={"row": peers[d]}, device_id_type=MESH)

    def back_in(d):
        return pltpu.make_async_remote_copy(
            src_ref=s2.at[peers[d]], dst_ref=r2.at[sources[d]],
            send_sem=back_send.at[d], recv_sem=back_recv.at[d],
            device_id={"row": peers[d]}, device_id_type=MESH)

    ld_tok.wait()
    sends = []
    first = lax.rem(row, half)

    def send(which, k):
        for i in range(k, half):
            target = order[k] * half + lax.rem(first + i, half)
            copy = out_copy(which, target, k * half + i)
            copy.start()
            sends.append(copy)

    for k in range(2):
        for copy in ld_half[k]:
            copy.wait()
        if k == 0:
            ld_wb = load(5, wb_h, wb)
            ld_fhi, ld_flo = load(6, fhi_h, fhi), load(7, flo_h, flo)
            small = [
                load(12 + i, src, dst)
                for i, (src, dst) in enumerate([
                    (own_taps_h, own_taps), (gate_taps_h, gate_taps), (pw_h, pw), (pb_h, pb),
                    (sf_h, sf), (hw_h, hw), (hb_h, hb), (fb_h, fb), (ld_h, ld)])
            ]
        made = dot(tok[...], wva[k]).astype(BF16)
        for which in range(2):
            for i in range(half):
                base = which * H + i * C
                sbuf[which, order[k] * half + i] = made[:, base : base + C]
        if k == 0:
            pl.semaphore_wait(barrier, R - 1)
            send(0, 0)
    send(0, 1)
    send(1, 0)
    send(1, 1)
    for which in range(2):
        rbuf[which, row] = sbuf[which, row]
    if aligned:
        wf_src = wf_h.at[:, :, :, pl.ds(pl.multiple_of(row * C, 128), C)]
    else:
        wf_src = wf_h
    ld_wf = load(8, wf_src, wf)
    ld_fcat, ld_twist, ld_gcat = load(9, fcat_h, fcat), load(10, twist_h, twist), load(11, gcat_h, gcat)
    ld_wb.wait()
    gb[...] = dot(tok[...], wb[...]).astype(BF16)
    for side in range(2):
        halo_copy(side).start()

    for copy in small:
        copy.wait()
    pwb[...] = jnp.zeros_like(pwb)
    pwb[0:PE, 0:HID] = pw[...]
    pwb[HID : HID + PE, HID : 2 * HID] = pw[...]
    hwb[...] = jnp.zeros_like(hwb)
    hwb[0:HID, 0:HID] = hw[...]
    hwb[HID : 2 * HID, HID : 2 * HID] = hw[...]
    wfb[...] = jnp.zeros_like(wfb)
    ld_wf.wait()
    for o in range(2):
        wfb[0:HID, o * C : (o + 1) * C] = wf[:, o, 0, :]
        wfb[HID : 2 * HID, (2 + o) * C : (3 + o) * C] = wf[:, o, 1, :]
    ld_fhi.wait()
    ld_flo.wait()

    def twice(v):
        return jnp.concatenate([v, v], axis=-1)

    decay = ld[:, own_at]
    rows_f = 256
    pb2, hb2, sf2 = twice(pb[...]), twice(hb[...]), twice(sf[...])

    def filter_rows(step, carry):
        at = pl.ds(pl.multiple_of(step * rows_f, rows_f), rows_f)
        pre = dot3((fhi[at, :], flo[at, :]), split(pwb[...])) + pb2
        ha = sine(sf2[0:1] * pre)
        pre = dot3(split(ha), split(hwb[...])) + hb2
        hb_ = sine(sf2[1:2] * pre)
        raw = dot3(split(hb_), split(wfb[...]))
        index = (lax.broadcasted_iota(jnp.int32, (rows_f, C), 0) + step * rows_f).astype(F32)
        scale = 1.0 / max(N - 1, 1)
        env_f = jnp.exp(-(index * scale) * decay) + WINDOW_SHIFT
        env_b = jnp.exp(-((N - index) * scale) * decay) + WINDOW_SHIFT
        env_b = jnp.where(index > 0.0, -env_b, 0.0)
        for o in range(2):
            kre[o, at, :] = raw[:, o * C : (o + 1) * C] * env_f
            kim[o, at, :] = raw[:, (2 + o) * C : (3 + o) * C] * env_b
        return carry

    lax.fori_loop(0, N // rows_f, filter_rows, 0)
    ld_fcat.wait()
    ld_twist.wait()
    ld_gcat.wait()

    def put_leaves(leaves, at, exact):
        for j, (re, im) in enumerate(leaves):
            tat = pl.ds(pl.multiple_of(j * LEAF + at, CHUNK), CHUNK)
            tc, ts = twist[0, tat, :], twist[1, tat, :]
            zr, zi = re * tc - im * ts, re * ts + im * tc
            lanes = slice(j * C, (j + 1) * C)
            for part, base in ((zr, 0), (zi, LEAF)):
                pat = pl.ds(pl.multiple_of(base + at, CHUNK), CHUNK)
                if exact:
                    xhi[pat, lanes], xlo[pat, lanes] = split(part)
                else:
                    xhi[pat, lanes] = part.astype(BF16)

    def get_leaves(at):
        leaves = []
        for j in range(L):
            tat = pl.ds(pl.multiple_of(j * LEAF + at, CHUNK), CHUNK)
            tc, ts = twist[0, tat, :], twist[1, tat, :]
            lanes = slice(j * C, (j + 1) * C)
            zr = ybuf[pl.ds(pl.multiple_of(at, CHUNK), CHUNK), lanes]
            zi = ybuf[pl.ds(pl.multiple_of(LEAF + at, CHUNK), CHUNK), lanes]
            leaves.append((zr * tc + zi * ts, zi * tc - zr * ts))
        return leaves

    width = 256 if (L * C) % 256 == 0 else L * C
    K2 = 2 * LEAF

    def mul3(cat, hi, lo):
        both = dot(cat[...], hi)
        return both[:K2] + both[K2:] + dot(cat[0:K2], lo)

    steps = LEAF // CHUNK

    def rows_at(n1, at):
        return pl.ds(pl.multiple_of(n1 * LEAF + at, CHUNK), CHUNK)

    for o in range(2):
        def kernel_in(step, carry, o=o):
            at = step * CHUNK
            blocks = [(kre[o, rows_at(n1, at), :], kim[o, rows_at(n1, at), :]) for n1 in range(L)]
            put_leaves(split_tree(blocks, math.pi / 2), at, True)
            return carry

        lax.fori_loop(0, steps, kernel_in, 0)
        for tile in range(L * C // width):
            lanes = slice(tile * width, (tile + 1) * width)
            spec[o, :, lanes] = mul3(fcat, xhi[:, lanes], xlo[:, lanes])

    def through(o, exact):
        for tile in range(L * C // width):
            lanes = slice(tile * width, (tile + 1) * width)
            if exact:
                z = mul3(fcat, xhi[:, lanes], xlo[:, lanes])
            else:
                z = dot(fcat[0:K2], xhi[:, lanes])
            zr, zi = z[:LEAF], z[LEAF:]
            kr, ki = spec[o, 0:LEAF, lanes], spec[o, LEAF:K2, lanes]
            y = jnp.concatenate([zr * kr - zi * ki, zr * ki + zi * kr], axis=0)
            if exact:
                ybuf[:, lanes] = mul3(gcat, *split(y))
            else:
                ybuf[:, lanes] = dot(gcat[0:K2], y.astype(BF16))

    def short(which, dest):
        for d in range(1, R):
            in_copy(which, d).wait_recv()
        pad[0:8] = jnp.zeros((8, C), F32)
        pad[8 + N : 16 + N] = jnp.zeros((8, C), F32)
        for r in range(R):
            pad[8 + r * T : 8 + (r + 1) * T] = rbuf[which, r].astype(F32)
        taps = own_taps[which, :, own_at].astype(F32)
        for r in range(R):
            a = r * T
            dest[a : a + T] = (
                taps[0:1] * pad[7 + a : 7 + a + T]
                + taps[1:2] * pad[8 + a : 8 + a + T]
                + taps[2:3] * pad[9 + a : 9 + a + T]
            ).astype(BF16).astype(F32)

    short(0, xs)
    bias = fb[:, own_at]

    def value_in(step, carry):
        at = step * CHUNK
        blocks = [(xs[rows_at(n1, at), :], None) for n1 in range(L)]
        put_leaves(split_tree(blocks, math.pi / 2), at, True)
        return carry

    lax.fori_loop(0, steps, value_in, 0)
    through(0, True)
    short(1, gs)

    def middle(step, carry):
        at = step * CHUNK
        convolved = join_tree(get_leaves(at), math.pi / 2, True)
        blocks = []
        for n1 in range(L):
            here = rows_at(n1, at)
            gated = gs[here, :] * (convolved[n1] + bias[0:1] * xs[here, :])
            xs[here, :] = gated
            blocks.append((gated, None))
        put_leaves(split_tree(blocks, math.pi / 2), at, False)
        return carry

    lax.fori_loop(0, steps, middle, 0)
    through(1, False)

    def last(step, carry):
        at = step * CHUNK
        convolved = join_tree(get_leaves(at), math.pi / 2, True)
        for n1 in range(L):
            value = convolved[n1] + bias[1:2] * xs[rows_at(n1, at), :]
            r, inner = (n1 * LEAF) // T, (n1 * LEAF) % T
            s2[r, pl.ds(pl.multiple_of(inner + at, CHUNK), CHUNK), :] = value.astype(BF16)
        return carry

    lax.fori_loop(0, steps, last, 0)
    for d in [half] + [d for d in range(1, R) if d != half]:
        back_out(d).start()
    r2[row] = s2[row]

    for side in range(2):
        halo_copy(side).wait_recv()
    before = halo[0, CHUNK - 8 : CHUNK].astype(F32)
    after = halo[1, 0:8].astype(F32)
    gpad[0:8] = jnp.where(row > 0, before, 0.0)
    gpad[8 : 8 + T] = gb[...].astype(F32)
    gpad[8 + T : 16 + T] = jnp.where(row < R - 1, after, 0.0)
    taps = gate_taps[2, :, share_at].astype(F32)
    gbs[...] = (
        taps[0:1] * gpad[7 : 7 + T] + taps[1:2] * gpad[8 : 8 + T] + taps[2:3] * gpad[9 : 9 + T]
    ).astype(BF16).astype(F32)
    for d in range(1, R):
        back_in(d).wait_recv()
    for r in range(R):
        lanes = slice(r * C, (r + 1) * C)
        out_ref[:, lanes] = (gbs[:, lanes] * r2[r].astype(F32)).astype(BF16)
    for copy in sends:
        copy.wait_send()
    for d in range(1, R):
        back_out(d).wait_send()
    for side in range(2):
        halo_copy(side).wait_send()


def per_device(
    tokens, w_value, w_gate_a, w_gate_b, short_taps, pos_weight, pos_bias, sine_freq,
    hid_weight, hid_bias, filter_out, filter_bias, lag_decay,
):
    R = lax.axis_size("row")
    T, D = tokens.shape
    N = T * R
    S = w_value.shape[1]
    C = S // R
    PE, HID = pos_weight.shape
    L = N // LEAF
    row, col = lax.axis_index("row"), lax.axis_index("col")
    fcat, gcat, twist, fhi, flo = tables(N, C, PE, HID)
    own_w = filter_out
    own_taps, gate_taps, fb, ld = short_taps, short_taps, filter_bias, lag_decay[None]
    if C % 128:
        own_w = lax.dynamic_slice_in_dim(own_w, row * C, C, 3)
        start = col * S + row * C
        own_taps = lax.dynamic_slice_in_dim(own_taps, start, C, 2)
        gate_taps = lax.dynamic_slice_in_dim(gate_taps, col * S, S, 2)
        fb = lax.dynamic_slice_in_dim(fb, start, C, 1)
        ld = lax.dynamic_slice_in_dim(ld, start, C, 1)
    vm = pl.BlockSpec(memory_space=pltpu.VMEM)
    hbm = pl.BlockSpec(memory_space=pl.ANY)
    dma = pltpu.SemaphoreType.DMA
    small = [own_taps, gate_taps, pos_weight, pos_bias[None], sine_freq, hid_weight, hid_bias[None], fb, ld]
    return pl.pallas_call(
        functools.partial(kernel, (R, T, N, C, S, HID, PE)),
        out_shape=jax.ShapeDtypeStruct((T, S), BF16),
        in_specs=[hbm] * 19,
        out_specs=vm,
        scratch_shapes=[pltpu.VMEM(x.shape, x.dtype) for x in small] + [
            pltpu.VMEM((T, D), BF16),
            pltpu.VMEM((2, D, S), BF16),
            pltpu.VMEM((D, S), BF16),
            pltpu.VMEM(fcat.shape, BF16),
            pltpu.VMEM(gcat.shape, BF16),
            pltpu.VMEM(twist.shape, F32),
            pltpu.VMEM(fhi.shape, BF16),
            pltpu.VMEM(flo.shape, BF16),
            pltpu.VMEM((HID, 2, 2, C), F32),
            pltpu.VMEM((2, R, T, C), BF16),
            pltpu.VMEM((2, R, T, C), BF16),
            pltpu.VMEM((T, S), BF16),
            pltpu.VMEM((2, CHUNK, S), BF16),
            pltpu.VMEM((N + 16, C), F32),
            pltpu.VMEM((N, C), F32),
            pltpu.VMEM((N, C), F32),
            pltpu.VMEM((T + 16, S), F32),
            pltpu.VMEM((T, S), F32),
            pltpu.VMEM((2 * HID, 2 * HID), F32),
            pltpu.VMEM((2 * HID, 2 * HID), F32),
            pltpu.VMEM((2 * HID, 4 * C), F32),
            pltpu.VMEM((2, N, C), F32),
            pltpu.VMEM((2, N, C), F32),
            pltpu.VMEM((2 * LEAF, L * C), BF16),
            pltpu.VMEM((2 * LEAF, L * C), BF16),
            pltpu.VMEM((2, 2 * LEAF, L * C), F32),
            pltpu.VMEM((2 * LEAF, L * C), F32),
            pltpu.VMEM((R, T, C), BF16),
            pltpu.VMEM((R, T, C), BF16),
            dma((21,)),
            dma((2, R)),
            dma((2, R)),
            dma((2,)),
            dma((2,)),
            dma((R,)),
            dma((R,)),
        ],
        compiler_params=pltpu.CompilerParams(
            collective_id=0, has_side_effects=True, vmem_limit_bytes=44 * 1024 * 1024
        ),
    )(*[
        pltpu.with_memory_space_constraint(jnp.asarray(x), pltpu.HBM)
        for x in (tokens, w_value, w_gate_a, w_gate_b, fcat, gcat, twist, fhi, flo, own_w, *small)
    ])


def solution(mesh):
    in_specs = (
        P(("grp", "row"), None), P(None, "col"), P(None, "col"), P(None, "col"),
        P(), P(), P(), P(), P(), P(), P(None, None, None, "col"), P(), P(),
    )
    return jax.shard_map(
        per_device, mesh=mesh, in_specs=in_specs, out_specs=P(("grp", "row"), "col"), check_vma=False
    )
```

```python
import functools
import math

import jax
import jax.numpy as jnp
import numpy as np
from jax import lax
from jax.experimental import pallas as pl
from jax.experimental.pallas import tpu as pltpu
from jax.sharding import PartitionSpec as P

WINDOW_SHIFT = 0.05
LEAF = 128
CHUNK = 16
PIECE = 64
EXACT = False
MESH = pl.DeviceIdType.MESH
F32 = jnp.float32
BF16 = jnp.bfloat16


def leaf_angles(theta, count):
    if count == 1:
        return [theta]
    half = theta / 2
    return leaf_angles(half, count // 2) + leaf_angles(half + math.pi, count // 2)


def split_np(values):
    high = values.astype(jnp.bfloat16)
    low = (values - high.astype(np.float64)).astype(jnp.bfloat16)
    return high, low


@functools.lru_cache(maxsize=None)
def tables(seq, lanes, features, hidden):
    k = np.arange(LEAF)
    angle = 2 * np.pi / LEAF * ((k[:, None] * k[None, :]) % LEAF)
    cos, sin = np.cos(angle), np.sin(angle)
    forward = np.block([[cos, -sin], [sin, cos]])
    inverse = np.block([[cos, sin], [-sin, cos]]) / seq
    fcat = np.concatenate(split_np(forward), axis=0)
    gcat = np.concatenate(split_np(inverse), axis=0)
    thetas = np.array(leaf_angles(math.pi / 2, seq // LEAF))
    twist = (thetas[:, None] * k[None, :] / LEAF).reshape(-1)
    twist = np.stack([np.cos(twist), np.sin(twist)]).astype(np.float32)
    twist = np.ascontiguousarray(np.broadcast_to(twist[:, :, None], (2, seq, lanes)))
    bands = (features - 1) // 2
    freq = np.linspace(0.0001, bands - 1, bands, dtype=np.float32)

    def feats(positions):
        positions = positions.astype(np.float32)
        scaled = positions / np.float32(max(seq - 1, 1))
        ang = (np.float32(2.0 * math.pi / seq) * positions)[:, None] * freq[None, :]
        ang = ang.astype(np.float64)
        return np.concatenate([scaled[:, None], np.cos(ang), -np.sin(ang)], axis=1)

    both = np.zeros((seq, 2 * hidden))
    both[:, :features] = feats(np.arange(seq))
    both[:, hidden : hidden + features] = feats(seq - np.arange(seq))
    feat = np.concatenate(split_np(both), axis=1)
    return fcat, gcat, twist, feat


def split(x):
    high = x.astype(BF16)
    return high, (x - high.astype(F32)).astype(BF16)


def dot(a, b):
    return jnp.dot(a, b, preferred_element_type=F32)


def deep(a, b):
    half = b.shape[0] // 2
    return dot(a[:, :half], b[:half]) + dot(a[:, half:], b[half:])


PI_A = 3.140625
PI_B = float(np.float32(math.pi - 3.140625))
PI_C = float(math.pi - 3.140625 - np.float32(math.pi - 3.140625))


def sine(x):
    k = jnp.floor(x * (1.0 / math.pi) + 0.5)
    r = x - k * PI_A
    r = r - k * PI_B
    r = r - k * PI_C
    parity = k - 2.0 * jnp.floor(k * 0.5)
    s = r * r
    p = -1.0 / 39916800.0
    for c in (1.0 / 362880.0, -1.0 / 5040.0, 1.0 / 120.0, -1.0 / 6.0):
        p = p * s + c
    return (r + r * s * p) * (1.0 - 2.0 * parity)


def split_tree(blocks, theta):
    if len(blocks) == 1:
        return blocks
    half = len(blocks) // 2
    wr, wi = math.cos(theta / 2), math.sin(theta / 2)
    up, down = [], []
    for (ar, ai), (br, bi) in zip(blocks[:half], blocks[half:]):
        if bi is None:
            tr, ti = br * wr, br * wi
            up.append((ar + tr, ti))
            down.append((ar - tr, -ti))
        else:
            tr, ti = br * wr - bi * wi, br * wi + bi * wr
            up.append((ar + tr, ai + ti))
            down.append((ar - tr, ai - ti))
    return split_tree(up, theta / 2) + split_tree(down, theta / 2 + math.pi)


def join_tree(leaves, theta, top):
    if len(leaves) == 1:
        return leaves
    half = len(leaves) // 2
    up = join_tree(leaves[:half], theta / 2, False)
    down = join_tree(leaves[half:], theta / 2 + math.pi, False)
    wr, wi = math.cos(theta / 2), math.sin(theta / 2)
    first, second = [], []
    for (pr, pi), (qr, qi) in zip(up, down):
        dr, di = pr - qr, pi - qi
        if top:
            first.append(pr + qr)
            second.append(dr * wr + di * wi)
        else:
            first.append((pr + qr, pi + qi))
            second.append((dr * wr + di * wi, di * wr - dr * wi))
    return first + second


def kernel(
    sizes,
    tok_h, wv_h, wa_h, wb_h, fcat_h, gcat_h, twist_h, feat_h,
    wf_h, own_taps_h, gate_taps_h, pw_h, pb_h, sf_h, hw_h, hb_h, fb_h, ld_h,
    out_ref,
    own_taps, gate_taps, pw, pb, sf, hw, hb, fb, ld,
    tok, acc, wva, wb, fcat, gcat, twist, feat,
    wf, sbuf, rbuf, gb, halo, pad, xs, gpad, gbs,
    pwb, hwb, w1, w2, w3, kre, kim, xhi, xlo, spec, ybuf, s2, r2,
    in_sem, send_sem, recv_sem, halo_send, halo_recv, back_send, back_recv,
):
    R, T, N, C, S, HID, PE = sizes
    D = tok.shape[1]
    L = N // LEAF
    row = lax.axis_index("row")
    col = lax.axis_index("col")
    aligned = C % 128 == 0
    if aligned:
        own_at = pl.ds(pl.multiple_of(col * S + row * C, 128), C)
        share_at = pl.ds(pl.multiple_of(col * S, 128), S)
    else:
        own_at, share_at = slice(0, C), slice(0, S)

    half = R // 2
    H = S // 2
    low = row < half
    inner = jnp.logical_and(row > 0, row < R - 1)
    first = lax.rem(row, half)
    far = [jnp.where(low, half + i, half - 1 - i) for i in range(half)]
    near = [jnp.where(low, 0, half) + lax.rem(first + i, half) for i in range(1, half)]
    order = [jnp.where(low, 1, 0), jnp.where(low, 0, 1)]

    def load(i, src, dst):
        copy = pltpu.make_async_copy(src, dst, in_sem.at[i])
        copy.start()
        return copy

    def load_half(i, src, which, k, rows=slice(None)):
        lanes = pl.ds(pl.multiple_of(order[k] * H, H), H)
        return load(i, src.at[rows, lanes], wva.at[k, rows, which * H : (which + 1) * H])

    halves = [slice(0, D // 2), slice(D // 2, D)]
    ld_first = []
    for i, part in enumerate(halves):
        ld_first.append([
            load(2 * i, tok_h.at[:, part], tok.at[:, part]),
            load_half(2 * i + 1, wv_h, 0, 0, part),
        ])

    barrier = pltpu.get_barrier_semaphore()
    peers = [lax.rem(row + d, R) for d in range(R)]
    sources = [lax.rem(row + R - d, R) for d in range(R)]
    for d in range(1, R):
        pl.semaphore_signal(barrier, inc=1, device_id={"row": peers[d]}, device_id_type=MESH)

    def pieces(total, size):
        return [pl.ds(at, size) for at in range(0, total, size)]

    def out_copy(which, target, slot, part):
        return pltpu.make_async_remote_copy(
            src_ref=sbuf.at[which, target, part], dst_ref=rbuf.at[which, row, part],
            send_sem=send_sem.at[which, slot], recv_sem=recv_sem.at[which, row],
            device_id={"row": target}, device_id_type=MESH)

    def in_copy(which, d):
        return pltpu.make_async_remote_copy(
            src_ref=sbuf.at[which, peers[d]], dst_ref=rbuf.at[which, sources[d]],
            send_sem=send_sem.at[which, d - 1], recv_sem=recv_sem.at[which, sources[d]],
            device_id={"row": peers[d]}, device_id_type=MESH)

    def halo_copy(side):
        src = gb.at[pl.ds(T - CHUNK, CHUNK)] if side == 0 else gb.at[pl.ds(0, CHUNK)]
        target = peers[1] if side == 0 else peers[R - 1]
        return pltpu.make_async_remote_copy(
            src_ref=src, dst_ref=halo.at[side],
            send_sem=halo_send.at[side], recv_sem=halo_recv.at[side],
            device_id={"row": target}, device_id_type=MESH)

    def back_out(j, part):
        a, b = (far + near)[j], (near + far)[j]
        target = jnp.where(inner, a, b)
        return pltpu.make_async_remote_copy(
            src_ref=s2.at[target, part], dst_ref=r2.at[row, part],
            send_sem=back_send.at[j], recv_sem=back_recv.at[row],
            device_id={"row": target}, device_id_type=MESH)

    def back_in(d):
        return pltpu.make_async_remote_copy(
            src_ref=s2.at[peers[d]], dst_ref=r2.at[sources[d]],
            send_sem=back_send.at[d - 1], recv_sem=back_recv.at[sources[d]],
            device_id={"row": peers[d]}, device_id_type=MESH)

    def send(which, k):
        for slot, target in enumerate(near if k else far):
            for part in pieces(T, min(PIECE, T)):
                out_copy(which, target, slot + (half if k else 0), part).start()

    def keep(which, k, made):
        for i in range(half):
            sbuf[which, order[k] * half + i] = made[:, i * C : (i + 1) * C]

    for copy in ld_first[0]:
        copy.wait()
    ld_near = [load_half(5 + which, src, which, 1) for which, src in enumerate((wv_h, wa_h))]
    ld_far_a = load_half(4, wa_h, 1, 0)
    small = [
        load(12 + i, src, dst)
        for i, (src, dst) in enumerate([
            (own_taps_h, own_taps), (gate_taps_h, gate_taps), (pw_h, pw), (pb_h, pb),
            (sf_h, sf), (hw_h, hw), (hb_h, hb), (fb_h, fb), (ld_h, ld)])
    ]
    if aligned:
        wf_src = wf_h.at[:, :, :, pl.ds(pl.multiple_of(row * C, 128), C)]
    else:
        wf_src = wf_h
    ld_wf = load(8, wf_src, wf)
    ld_wb = load(7, wb_h, wb)
    ld_feat = load(21, feat_h, feat)
    acc[...] = deep(tok[:, halves[0]], wva[0, halves[0], 0:H])
    for copy in ld_first[1]:
        copy.wait()
    acc[...] += deep(tok[:, halves[1]], wva[0, halves[1], 0:H])
    keep(0, 0, acc[...].astype(BF16))

    @pl.when(inner)
    def _():
        pl.semaphore_wait(barrier, R - 1)
        send(0, 0)

    for copy in ld_near:
        copy.wait()
    made = dot(tok[...], wva[1]).astype(BF16)
    keep(0, 1, made[:, 0:H])
    keep(1, 1, made[:, H : 2 * H])

    @pl.when(jnp.logical_not(inner))
    def _():
        pl.semaphore_wait(barrier, R - 1)
        send(0, 1)
        send(0, 0)

    ld_far_a.wait()
    keep(1, 0, deep(tok[...], wva[0, :, H : 2 * H]).astype(BF16))

    @pl.when(inner)
    def _():
        send(1, 0)
        send(0, 1)
        send(1, 1)

    @pl.when(jnp.logical_not(inner))
    def _():
        send(1, 1)
        send(1, 0)

    for which in range(2):
        rbuf[which, row] = sbuf[which, row]
    ld_fcat, ld_twist, ld_gcat = load(9, fcat_h, fcat), load(10, twist_h, twist), load(11, gcat_h, gcat)
    for copy in small:
        copy.wait()
    W = 2 * HID
    pwb[...] = jnp.zeros_like(pwb)
    pwb[0:PE, 0:HID] = pw[...]
    pwb[HID : HID + PE, HID : 2 * HID] = pw[...]
    hwb[...] = jnp.zeros_like(hwb)
    hwb[0:HID, 0:HID] = hw[...]
    hwb[HID : 2 * HID, HID : 2 * HID] = hw[...]
    for w, full in ((w1, pwb), (w2, hwb)):
        high, low = split(full[...])
        w[0:W, 0:W] = high
        w[0:W, W : 2 * W] = low
        w[W : 2 * W, 0:W] = high
        w[W : 2 * W, W : 2 * W] = jnp.zeros_like(low)
    ld_wf.wait()
    for o in range(2):
        for way in range(2):
            high, low = split(wf[:, o, way, :])
            for at, part in enumerate((high, high, low, low)):
                w3[way, at * HID : (at + 1) * HID, o * C : (o + 1) * C] = part
    ld_feat.wait()

    def twice(v):
        return jnp.concatenate([v, v], axis=-1)

    decay = ld[:, own_at]
    rows_f = 256
    pb2, hb2, sf2 = twice(pb[...]), twice(hb[...]), twice(sf[...])

    def filter_rows(step, carry):
        at = pl.ds(pl.multiple_of(step * rows_f, rows_f), rows_f)
        both = dot(feat[at, :], w1[...])
        ha = sine(sf2[0:1] * (both[:, 0:W] + both[:, W : 2 * W] + pb2))
        both = dot(jnp.concatenate(split(ha), axis=-1), w2[...])
        hb_ = sine(sf2[1:2] * (both[:, 0:W] + both[:, W : 2 * W] + hb2))
        swapped = pltpu.roll(hb_, HID, 1)
        lower = lax.broadcasted_iota(jnp.int32, (rows_f, W), 1) < HID
        raw = []
        for way, (head, tail) in enumerate(((hb_, swapped), (swapped, hb_))):
            part = jnp.where(lower, head, tail - tail.astype(BF16).astype(F32)).astype(BF16)
            raw.append(dot(jnp.concatenate([part, part], axis=-1), w3[way]))
        index = (lax.broadcasted_iota(jnp.int32, (rows_f, C), 0) + step * rows_f).astype(F32)
        scale = 1.0 / max(N - 1, 1)
        env_f = jnp.exp(-(index * scale) * decay) + WINDOW_SHIFT
        env_b = jnp.exp(-((N - index) * scale) * decay) + WINDOW_SHIFT
        env_b = jnp.where(index > 0.0, -env_b, 0.0)
        for o in range(2):
            kre[o, at, :] = raw[0][:, o * C : (o + 1) * C] * env_f
            kim[o, at, :] = raw[1][:, o * C : (o + 1) * C] * env_b
        return carry

    lax.fori_loop(0, N // rows_f, filter_rows, 0, unroll=2)
    ld_fcat.wait()
    ld_twist.wait()
    ld_gcat.wait()

    def put_leaves(leaves, at, exact):
        for j, (re, im) in enumerate(leaves):
            tat = pl.ds(pl.multiple_of(j * LEAF + at, CHUNK), CHUNK)
            tc, ts = twist[0, tat, :], twist[1, tat, :]
            zr, zi = re * tc - im * ts, re * ts + im * tc
            lanes = slice(j * C, (j + 1) * C)
            for part, base in ((zr, 0), (zi, LEAF)):
                pat = pl.ds(pl.multiple_of(base + at, CHUNK), CHUNK)
                if exact:
                    xhi[pat, lanes], xlo[pat, lanes] = split(part)
                else:
                    xhi[pat, lanes] = part.astype(BF16)

    def get_leaves(at):
        leaves = []
        for j in range(L):
            tat = pl.ds(pl.multiple_of(j * LEAF + at, CHUNK), CHUNK)
            tc, ts = twist[0, tat, :], twist[1, tat, :]
            lanes = slice(j * C, (j + 1) * C)
            zr = ybuf[pl.ds(pl.multiple_of(at, CHUNK), CHUNK), lanes]
            zi = ybuf[pl.ds(pl.multiple_of(LEAF + at, CHUNK), CHUNK), lanes]
            leaves.append((zr * tc + zi * ts, zi * tc - zr * ts))
        return leaves

    width = 256 if (L * C) % 256 == 0 else L * C
    K2 = 2 * LEAF

    def mul3(cat, hi, lo):
        both = dot(cat[...], hi)
        return both[:K2] + both[K2:] + dot(cat[0:K2], lo)

    steps = LEAF // CHUNK

    def rows_at(n1, at):
        return pl.ds(pl.multiple_of(n1 * LEAF + at, CHUNK), CHUNK)

    for o in range(2):
        def kernel_in(step, carry, o=o):
            at = step * CHUNK
            blocks = [(kre[o, rows_at(n1, at), :], kim[o, rows_at(n1, at), :]) for n1 in range(L)]
            put_leaves(split_tree(blocks, math.pi / 2), at, EXACT)
            return carry

        lax.fori_loop(0, steps, kernel_in, 0)
        for tile in range(L * C // width):
            lanes = slice(tile * width, (tile + 1) * width)
            if EXACT:
                spec[o, :, lanes] = mul3(fcat, xhi[:, lanes], xlo[:, lanes])
            else:
                spec[o, :, lanes] = dot(fcat[0:K2], xhi[:, lanes])

    def through(o, exact):
        for tile in range(L * C // width):
            lanes = slice(tile * width, (tile + 1) * width)
            if exact:
                z = mul3(fcat, xhi[:, lanes], xlo[:, lanes])
            else:
                z = dot(fcat[0:K2], xhi[:, lanes])
            zr, zi = z[:LEAF], z[LEAF:]
            kr, ki = spec[o, 0:LEAF, lanes], spec[o, LEAF:K2, lanes]
            y = jnp.concatenate([zr * kr - zi * ki, zr * ki + zi * kr], axis=0)
            if exact:
                ybuf[:, lanes] = mul3(gcat, *split(y))
            else:
                ybuf[:, lanes] = dot(gcat[0:K2], y.astype(BF16))

    def short(which):
        pad[0:8] = jnp.zeros((8, C), F32)
        pad[8 + N : 16 + N] = jnp.zeros((8, C), F32)
        for r in range(R):
            pad[8 + r * T : 8 + (r + 1) * T] = rbuf[which, r].astype(F32)
        taps = own_taps[which, :, own_at].astype(F32)
        for r in range(R):
            a = r * T
            made = (
                taps[0:1] * pad[7 + a : 7 + a + T]
                + taps[1:2] * pad[8 + a : 8 + a + T]
                + taps[2:3] * pad[9 + a : 9 + a + T]
            ).astype(BF16).astype(F32)
            xs[a : a + T] = made if which == 0 else made * xs[a : a + T]

    for d in range(1, R):
        in_copy(0, d).wait_recv()

    short(0)
    bias = fb[:, own_at]

    def signal_in(exact):
        def body(step, carry):
            at = step * CHUNK
            blocks = [(xs[rows_at(n1, at), :], None) for n1 in range(L)]
            put_leaves(split_tree(blocks, math.pi / 2), at, exact)
            return carry

        lax.fori_loop(0, steps, body, 0)

    signal_in(EXACT)
    through(0, EXACT)

    def middle(step, carry):
        at = step * CHUNK
        convolved = join_tree(get_leaves(at), math.pi / 2, True)
        for n1 in range(L):
            here = rows_at(n1, at)
            xs[here, :] = convolved[n1] + bias[0:1] * xs[here, :]
        return carry

    lax.fori_loop(0, steps, middle, 0)
    ld_wb.wait()
    gb[...] = dot(tok[...], wb[...]).astype(BF16)
    for side in range(2):
        halo_copy(side).start()
    for d in range(1, R):
        in_copy(1, d).wait_recv()
    short(1)
    signal_in(False)
    through(1, False)

    def last(step, carry):
        at = step * CHUNK
        convolved = join_tree(get_leaves(at), math.pi / 2, True)
        for n1 in range(L):
            value = convolved[n1] + bias[1:2] * xs[rows_at(n1, at), :]
            r, inner = (n1 * LEAF) // T, (n1 * LEAF) % T
            s2[r, pl.ds(pl.multiple_of(inner + at, CHUNK), CHUNK), :] = value.astype(BF16)
        return carry

    for part in range(2):
        lax.fori_loop(part * steps // 2, (part + 1) * steps // 2, last, 0)
        for j in range(R - 1):
            for n1 in range(T // LEAF):
                back_out(j, pl.ds(n1 * LEAF + part * LEAF // 2, LEAF // 2)).start()
    r2[row] = s2[row]

    for side in range(2):
        halo_copy(side).wait_recv()
    before = halo[0, CHUNK - 8 : CHUNK].astype(F32)
    after = halo[1, 0:8].astype(F32)
    gpad[0:8] = jnp.where(row > 0, before, 0.0)
    gpad[8 : 8 + T] = gb[...].astype(F32)
    gpad[8 + T : 16 + T] = jnp.where(row < R - 1, after, 0.0)
    taps = gate_taps[2, :, share_at].astype(F32)
    gbs[...] = (
        taps[0:1] * gpad[7 : 7 + T] + taps[1:2] * gpad[8 : 8 + T] + taps[2:3] * gpad[9 : 9 + T]
    ).astype(BF16).astype(F32)
    for d in range(1, R):
        back_in(d).wait_recv()
    for r in range(R):
        lanes = slice(r * C, (r + 1) * C)
        out_ref[:, lanes] = (gbs[:, lanes] * r2[r].astype(F32)).astype(BF16)
    for d in range(1, R):
        for which in range(2):
            in_copy(which, d).wait_send()
        back_in(d).wait_send()
    for side in range(2):
        halo_copy(side).wait_send()


def per_device(
    tokens, w_value, w_gate_a, w_gate_b, short_taps, pos_weight, pos_bias, sine_freq,
    hid_weight, hid_bias, filter_out, filter_bias, lag_decay,
):
    R = lax.axis_size("row")
    T, D = tokens.shape
    N = T * R
    S = w_value.shape[1]
    C = S // R
    PE, HID = pos_weight.shape
    L = N // LEAF
    row, col = lax.axis_index("row"), lax.axis_index("col")
    fcat, gcat, twist, feat = tables(N, C, PE, HID)
    own_w = filter_out
    own_taps, gate_taps, fb, ld = short_taps, short_taps, filter_bias, lag_decay[None]
    if C % 128:
        own_w = lax.dynamic_slice_in_dim(own_w, row * C, C, 3)
        start = col * S + row * C
        own_taps = lax.dynamic_slice_in_dim(own_taps, start, C, 2)
        gate_taps = lax.dynamic_slice_in_dim(gate_taps, col * S, S, 2)
        fb = lax.dynamic_slice_in_dim(fb, start, C, 1)
        ld = lax.dynamic_slice_in_dim(ld, start, C, 1)
    vm = pl.BlockSpec(memory_space=pltpu.VMEM)
    hbm = pl.BlockSpec(memory_space=pl.ANY)
    dma = pltpu.SemaphoreType.DMA
    small = [own_taps, gate_taps, pos_weight, pos_bias[None], sine_freq, hid_weight, hid_bias[None], fb, ld]
    return pl.pallas_call(
        functools.partial(kernel, (R, T, N, C, S, HID, PE)),
        out_shape=jax.ShapeDtypeStruct((T, S), BF16),
        in_specs=[hbm] * 18,
        out_specs=vm,
        scratch_shapes=[pltpu.VMEM(x.shape, x.dtype) for x in small] + [
            pltpu.VMEM((T, D), BF16),
            pltpu.VMEM((T, S // 2), F32),
            pltpu.VMEM((2, D, S), BF16),
            pltpu.VMEM((D, S), BF16),
            pltpu.VMEM(fcat.shape, BF16),
            pltpu.VMEM(gcat.shape, BF16),
            pltpu.VMEM(twist.shape, F32),
            pltpu.VMEM(feat.shape, BF16),
            pltpu.VMEM((HID, 2, 2, C), F32),
            pltpu.VMEM((2, R, T, C), BF16),
            pltpu.VMEM((2, R, T, C), BF16),
            pltpu.VMEM((T, S), BF16),
            pltpu.VMEM((2, CHUNK, S), BF16),
            pltpu.VMEM((N + 16, C), F32),
            pltpu.VMEM((N, C), F32),
            pltpu.VMEM((T + 16, S), F32),
            pltpu.VMEM((T, S), F32),
            pltpu.VMEM((2 * HID, 2 * HID), F32),
            pltpu.VMEM((2 * HID, 2 * HID), F32),
            pltpu.VMEM((4 * HID, 4 * HID), BF16),
            pltpu.VMEM((4 * HID, 4 * HID), BF16),
            pltpu.VMEM((2, 4 * HID, 2 * C), BF16),
            pltpu.VMEM((2, N, C), F32),
            pltpu.VMEM((2, N, C), F32),
            pltpu.VMEM((2 * LEAF, L * C), BF16),
            pltpu.VMEM((2 * LEAF, L * C), BF16),
            pltpu.VMEM((2, 2 * LEAF, L * C), F32),
            pltpu.VMEM((2 * LEAF, L * C), F32),
            pltpu.VMEM((R, T, C), BF16),
            pltpu.VMEM((R, T, C), BF16),
            dma((22,)),
            dma((2, R)),
            dma((2, R)),
            dma((2,)),
            dma((2,)),
            dma((R,)),
            dma((R,)),
        ],
        compiler_params=pltpu.CompilerParams(
            collective_id=0, has_side_effects=True, vmem_limit_bytes=44 * 1024 * 1024
        ),
    )(*[
        pltpu.with_memory_space_constraint(jnp.asarray(x), pltpu.HBM)
        for x in (tokens, w_value, w_gate_a, w_gate_b, fcat, gcat, twist, feat, own_w, *small)
    ])


def solution(mesh):
    in_specs = (
        P(("grp", "row"), None), P(None, "col"), P(None, "col"), P(None, "col"),
        P(), P(), P(), P(), P(), P(), P(None, None, None, "col"), P(), P(),
    )
    return jax.shard_map(
        per_device, mesh=mesh, in_specs=in_specs, out_specs=P(("grp", "row"), "col"), check_vma=False
    )
```

```python
import functools
import math

import jax
import jax.numpy as jnp
import numpy as np
from jax import lax
from jax.experimental import pallas as pl
from jax.experimental.pallas import tpu as pltpu
from jax.sharding import PartitionSpec as P

WINDOW_SHIFT = 0.05
LEAF = 128
CHUNK = 16
PIECE = 256
EXACT = False
MESH = pl.DeviceIdType.MESH
F32 = jnp.float32
BF16 = jnp.bfloat16


def leaf_angles(theta, count):
    if count == 1:
        return [theta]
    half = theta / 2
    return leaf_angles(half, count // 2) + leaf_angles(half + math.pi, count // 2)


def split_np(values):
    high = values.astype(jnp.bfloat16)
    low = (values - high.astype(np.float64)).astype(jnp.bfloat16)
    return high, low


@functools.lru_cache(maxsize=None)
def tables(seq, lanes, features, hidden):
    k = np.arange(LEAF)
    angle = 2 * np.pi / LEAF * ((k[:, None] * k[None, :]) % LEAF)
    cos, sin = np.cos(angle), np.sin(angle)
    forward = np.block([[cos, -sin], [sin, cos]])
    inverse = np.block([[cos, sin], [-sin, cos]]) / seq
    fcat = np.concatenate(split_np(forward), axis=0)
    gcat = np.concatenate(split_np(inverse), axis=0)
    thetas = np.array(leaf_angles(math.pi / 2, seq // LEAF))
    twist = (thetas[:, None] * k[None, :] / LEAF).reshape(-1)
    twist = np.stack([np.cos(twist), np.sin(twist)]).astype(np.float32)
    twist = np.ascontiguousarray(np.broadcast_to(twist[:, :, None], (2, seq, lanes)))
    bands = (features - 1) // 2
    freq = np.linspace(0.0001, bands - 1, bands, dtype=np.float32)

    def feats(positions):
        positions = positions.astype(np.float32)
        scaled = positions / np.float32(max(seq - 1, 1))
        ang = (np.float32(2.0 * math.pi / seq) * positions)[:, None] * freq[None, :]
        ang = ang.astype(np.float64)
        return np.concatenate([scaled[:, None], np.cos(ang), -np.sin(ang)], axis=1)

    both = np.zeros((seq, 2 * hidden))
    both[:, :features] = feats(np.arange(seq))
    both[:, hidden : hidden + features] = feats(seq - np.arange(seq))
    feat = np.concatenate(split_np(both), axis=1)
    return fcat, gcat, twist, feat


def split(x):
    high = x.astype(BF16)
    return high, (x - high.astype(F32)).astype(BF16)


def dot(a, b):
    return jnp.dot(a, b, preferred_element_type=F32)


def deep(a, b):
    half = b.shape[0] // 2
    return dot(a[:, :half], b[:half]) + dot(a[:, half:], b[half:])


PI_A = 3.140625
PI_B = float(np.float32(math.pi - 3.140625))
PI_C = float(math.pi - 3.140625 - np.float32(math.pi - 3.140625))


def sine(x):
    k = jnp.floor(x * (1.0 / math.pi) + 0.5)
    r = x - k * PI_A
    r = r - k * PI_B
    r = r - k * PI_C
    parity = k - 2.0 * jnp.floor(k * 0.5)
    s = r * r
    p = -1.0 / 39916800.0
    for c in (1.0 / 362880.0, -1.0 / 5040.0, 1.0 / 120.0, -1.0 / 6.0):
        p = p * s + c
    return (r + r * s * p) * (1.0 - 2.0 * parity)


def split_tree(blocks, theta):
    if len(blocks) == 1:
        return blocks
    half = len(blocks) // 2
    wr, wi = math.cos(theta / 2), math.sin(theta / 2)
    up, down = [], []
    for (ar, ai), (br, bi) in zip(blocks[:half], blocks[half:]):
        if bi is None:
            tr, ti = br * wr, br * wi
            up.append((ar + tr, ti))
            down.append((ar - tr, -ti))
        else:
            tr, ti = br * wr - bi * wi, br * wi + bi * wr
            up.append((ar + tr, ai + ti))
            down.append((ar - tr, ai - ti))
    return split_tree(up, theta / 2) + split_tree(down, theta / 2 + math.pi)


def join_tree(leaves, theta, top):
    if len(leaves) == 1:
        return leaves
    half = len(leaves) // 2
    up = join_tree(leaves[:half], theta / 2, False)
    down = join_tree(leaves[half:], theta / 2 + math.pi, False)
    wr, wi = math.cos(theta / 2), math.sin(theta / 2)
    first, second = [], []
    for (pr, pi), (qr, qi) in zip(up, down):
        dr, di = pr - qr, pi - qi
        if top:
            first.append(pr + qr)
            second.append(dr * wr + di * wi)
        else:
            first.append((pr + qr, pi + qi))
            second.append((dr * wr + di * wi, di * wr - dr * wi))
    return first + second


def kernel(
    sizes,
    tok_h, wv_h, wa_h, wb_h, fcat_h, gcat_h, twist_h, feat_h,
    wf_h, own_taps_h, gate_taps_h, pw_h, pb_h, sf_h, hw_h, hb_h, fb_h, ld_h,
    out_ref,
    own_taps, gate_taps, pw, pb, sf, hw, hb, fb, ld,
    tok, acc, wva, wb, fcat, gcat, twist, feat,
    wf, sbuf, rbuf, gb, halo, pad, xs, gpad, gbs,
    pwb, hwb, w1, w2, w3, kre, kim, xhi, xlo, spec, ybuf, s2, r2,
    in_sem, send_sem, recv_sem, halo_send, halo_recv, back_send, back_recv,
):
    R, T, N, C, S, HID, PE = sizes
    D = tok.shape[1]
    L = N // LEAF
    row = lax.axis_index("row")
    col = lax.axis_index("col")
    aligned = C % 128 == 0
    if aligned:
        own_at = pl.ds(pl.multiple_of(col * S + row * C, 128), C)
        share_at = pl.ds(pl.multiple_of(col * S, 128), S)
    else:
        own_at, share_at = slice(0, C), slice(0, S)

    half = R // 2
    H = S // 2
    low = row < half
    inner = jnp.logical_and(row > 0, row < R - 1)
    first = lax.rem(row, half)
    far = [jnp.where(low, half + i, half - 1 - i) for i in range(half)]
    near = [jnp.where(low, 0, half) + lax.rem(first + i, half) for i in range(1, half)]
    order = [jnp.where(low, 1, 0), jnp.where(low, 0, 1)]

    def load(i, src, dst):
        copy = pltpu.make_async_copy(src, dst, in_sem.at[i])
        copy.start()
        return copy

    def load_half(i, src, which, k, rows=slice(None)):
        lanes = pl.ds(pl.multiple_of(order[k] * H, H), H)
        return load(i, src.at[rows, lanes], wva.at[k, rows, which * H : (which + 1) * H])

    halves = [slice(0, D // 2), slice(D // 2, D)]
    ld_first = []
    for i, part in enumerate(halves):
        ld_first.append([
            load(2 * i, tok_h.at[:, part], tok.at[:, part]),
            load_half(2 * i + 1, wv_h, 0, 0, part),
        ])

    barrier = pltpu.get_barrier_semaphore()
    peers = [lax.rem(row + d, R) for d in range(R)]
    sources = [lax.rem(row + R - d, R) for d in range(R)]
    for d in range(1, R):
        pl.semaphore_signal(barrier, inc=1, device_id={"row": peers[d]}, device_id_type=MESH)

    def pieces(total, size):
        return [pl.ds(at, size) for at in range(0, total, size)]

    def out_copy(which, target, slot, part):
        return pltpu.make_async_remote_copy(
            src_ref=sbuf.at[which, target, part], dst_ref=rbuf.at[which, row, part],
            send_sem=send_sem.at[which, slot], recv_sem=recv_sem.at[which, row],
            device_id={"row": target}, device_id_type=MESH)

    def in_copy(which, d):
        return pltpu.make_async_remote_copy(
            src_ref=sbuf.at[which, peers[d]], dst_ref=rbuf.at[which, sources[d]],
            send_sem=send_sem.at[which, d - 1], recv_sem=recv_sem.at[which, sources[d]],
            device_id={"row": peers[d]}, device_id_type=MESH)

    def halo_copy(side):
        src = gb.at[pl.ds(T - CHUNK, CHUNK)] if side == 0 else gb.at[pl.ds(0, CHUNK)]
        target = peers[1] if side == 0 else peers[R - 1]
        return pltpu.make_async_remote_copy(
            src_ref=src, dst_ref=halo.at[side],
            send_sem=halo_send.at[side], recv_sem=halo_recv.at[side],
            device_id={"row": target}, device_id_type=MESH)

    def back_out(j, part):
        target = (far + near)[j]
        return pltpu.make_async_remote_copy(
            src_ref=s2.at[target, part], dst_ref=r2.at[row, part],
            send_sem=back_send.at[j], recv_sem=back_recv.at[row],
            device_id={"row": target}, device_id_type=MESH)

    def back_in(d):
        return pltpu.make_async_remote_copy(
            src_ref=s2.at[peers[d]], dst_ref=r2.at[sources[d]],
            send_sem=back_send.at[d - 1], recv_sem=back_recv.at[sources[d]],
            device_id={"row": peers[d]}, device_id_type=MESH)

    def send(which, k):
        for slot, target in enumerate(near if k else far):
            for part in pieces(T, min(PIECE, T)):
                out_copy(which, target, slot + (half if k else 0), part).start()

    def keep(which, k, made):
        for i in range(half):
            sbuf[which, order[k] * half + i] = made[:, i * C : (i + 1) * C]

    for copy in ld_first[0]:
        copy.wait()
    ld_near = [load_half(5 + which, src, which, 1) for which, src in enumerate((wv_h, wa_h))]
    ld_far_a = load_half(4, wa_h, 1, 0)
    small = [
        load(12 + i, src, dst)
        for i, (src, dst) in enumerate([
            (own_taps_h, own_taps), (gate_taps_h, gate_taps), (pw_h, pw), (pb_h, pb),
            (sf_h, sf), (hw_h, hw), (hb_h, hb), (fb_h, fb), (ld_h, ld)])
    ]
    if aligned:
        wf_src = wf_h.at[:, :, :, pl.ds(pl.multiple_of(row * C, 128), C)]
    else:
        wf_src = wf_h
    ld_wf = load(8, wf_src, wf)
    ld_wb = load(7, wb_h, wb)
    ld_feat = load(21, feat_h, feat)
    acc[...] = deep(tok[:, halves[0]], wva[0, halves[0], 0:H])
    for copy in ld_first[1]:
        copy.wait()
    acc[...] += deep(tok[:, halves[1]], wva[0, halves[1], 0:H])
    keep(0, 0, acc[...].astype(BF16))

    @pl.when(inner)
    def _():
        pl.semaphore_wait(barrier, R - 1)
        send(0, 0)

    for copy in ld_near:
        copy.wait()
    made = dot(tok[...], wva[1]).astype(BF16)
    keep(0, 1, made[:, 0:H])
    keep(1, 1, made[:, H : 2 * H])

    @pl.when(jnp.logical_not(inner))
    def _():
        pl.semaphore_wait(barrier, R - 1)
        send(0, 1)
        send(0, 0)

    ld_far_a.wait()
    keep(1, 0, deep(tok[...], wva[0, :, H : 2 * H]).astype(BF16))

    @pl.when(inner)
    def _():
        send(0, 1)

    even = lax.rem(col, 2) == 0
    @pl.when(even)
    def _():
        send(1, 1)
        send(1, 0)

    for which in range(2):
        rbuf[which, row] = sbuf[which, row]
    ld_fcat, ld_twist, ld_gcat = load(9, fcat_h, fcat), load(10, twist_h, twist), load(11, gcat_h, gcat)
    for copy in small:
        copy.wait()
    W = 2 * HID
    pwb[...] = jnp.zeros_like(pwb)
    pwb[0:PE, 0:HID] = pw[...]
    pwb[HID : HID + PE, HID : 2 * HID] = pw[...]
    hwb[...] = jnp.zeros_like(hwb)
    hwb[0:HID, 0:HID] = hw[...]
    hwb[HID : 2 * HID, HID : 2 * HID] = hw[...]
    for w, full in ((w1, pwb), (w2, hwb)):
        high, low = split(full[...])
        w[0:W, 0:W] = high
        w[0:W, W : 2 * W] = low
        w[W : 2 * W, 0:W] = high
        w[W : 2 * W, W : 2 * W] = jnp.zeros_like(low)
    ld_wf.wait()
    for o in range(2):
        for way in range(2):
            high, low = split(wf[:, o, way, :])
            for at, part in enumerate((high, high, low, low)):
                w3[way, at * HID : (at + 1) * HID, o * C : (o + 1) * C] = part
    ld_feat.wait()

    def twice(v):
        return jnp.concatenate([v, v], axis=-1)

    decay = ld[:, own_at]
    rows_f = 256
    pb2, hb2, sf2 = twice(pb[...]), twice(hb[...]), twice(sf[...])

    def filter_rows(step, carry):
        at = pl.ds(pl.multiple_of(step * rows_f, rows_f), rows_f)
        both = dot(feat[at, :], w1[...])
        ha = sine(sf2[0:1] * (both[:, 0:W] + both[:, W : 2 * W] + pb2))
        both = dot(jnp.concatenate(split(ha), axis=-1), w2[...])
        hb_ = sine(sf2[1:2] * (both[:, 0:W] + both[:, W : 2 * W] + hb2))
        swapped = pltpu.roll(hb_, HID, 1)
        lower = lax.broadcasted_iota(jnp.int32, (rows_f, W), 1) < HID
        raw = []
        for way, (head, tail) in enumerate(((hb_, swapped), (swapped, hb_))):
            part = jnp.where(lower, head, tail - tail.astype(BF16).astype(F32)).astype(BF16)
            raw.append(dot(jnp.concatenate([part, part], axis=-1), w3[way]))
        index = (lax.broadcasted_iota(jnp.int32, (rows_f, C), 0) + step * rows_f).astype(F32)
        scale = 1.0 / max(N - 1, 1)
        env_f = jnp.exp(-(index * scale) * decay) + WINDOW_SHIFT
        env_b = jnp.exp(-((N - index) * scale) * decay) + WINDOW_SHIFT
        env_b = jnp.where(index > 0.0, -env_b, 0.0)
        for o in range(2):
            kre[o, at, :] = raw[0][:, o * C : (o + 1) * C] * env_f
            kim[o, at, :] = raw[1][:, o * C : (o + 1) * C] * env_b
        return carry

    lax.fori_loop(0, N // rows_f, filter_rows, 0, unroll=2)
    ld_fcat.wait()
    ld_twist.wait()
    ld_gcat.wait()

    def put_leaves(leaves, at, exact):
        for j, (re, im) in enumerate(leaves):
            tat = pl.ds(pl.multiple_of(j * LEAF + at, CHUNK), CHUNK)
            tc, ts = twist[0, tat, :], twist[1, tat, :]
            zr, zi = re * tc - im * ts, re * ts + im * tc
            lanes = slice(j * C, (j + 1) * C)
            for part, base in ((zr, 0), (zi, LEAF)):
                pat = pl.ds(pl.multiple_of(base + at, CHUNK), CHUNK)
                if exact:
                    xhi[pat, lanes], xlo[pat, lanes] = split(part)
                else:
                    xhi[pat, lanes] = part.astype(BF16)

    def get_leaves(at):
        leaves = []
        for j in range(L):
            tat = pl.ds(pl.multiple_of(j * LEAF + at, CHUNK), CHUNK)
            tc, ts = twist[0, tat, :], twist[1, tat, :]
            lanes = slice(j * C, (j + 1) * C)
            zr = ybuf[pl.ds(pl.multiple_of(at, CHUNK), CHUNK), lanes]
            zi = ybuf[pl.ds(pl.multiple_of(LEAF + at, CHUNK), CHUNK), lanes]
            leaves.append((zr * tc + zi * ts, zi * tc - zr * ts))
        return leaves

    width = 256 if (L * C) % 256 == 0 else L * C
    K2 = 2 * LEAF

    def mul3(cat, hi, lo):
        both = dot(cat[...], hi)
        return both[:K2] + both[K2:] + dot(cat[0:K2], lo)

    steps = LEAF // CHUNK

    def rows_at(n1, at):
        return pl.ds(pl.multiple_of(n1 * LEAF + at, CHUNK), CHUNK)

    for o in range(2):
        def kernel_in(step, carry, o=o):
            at = step * CHUNK
            blocks = [(kre[o, rows_at(n1, at), :], kim[o, rows_at(n1, at), :]) for n1 in range(L)]
            put_leaves(split_tree(blocks, math.pi / 2), at, EXACT)
            return carry

        lax.fori_loop(0, steps, kernel_in, 0)
        for tile in range(L * C // width):
            lanes = slice(tile * width, (tile + 1) * width)
            if EXACT:
                spec[o, :, lanes] = mul3(fcat, xhi[:, lanes], xlo[:, lanes])
            else:
                spec[o, :, lanes] = dot(fcat[0:K2], xhi[:, lanes])

    def through(o, exact):
        for tile in range(L * C // width):
            lanes = slice(tile * width, (tile + 1) * width)
            if exact:
                z = mul3(fcat, xhi[:, lanes], xlo[:, lanes])
            else:
                z = dot(fcat[0:K2], xhi[:, lanes])
            zr, zi = z[:LEAF], z[LEAF:]
            kr, ki = spec[o, 0:LEAF, lanes], spec[o, LEAF:K2, lanes]
            y = jnp.concatenate([zr * kr - zi * ki, zr * ki + zi * kr], axis=0)
            if exact:
                ybuf[:, lanes] = mul3(gcat, *split(y))
            else:
                ybuf[:, lanes] = dot(gcat[0:K2], y.astype(BF16))

    def short(which):
        pad[0:8] = jnp.zeros((8, C), F32)
        pad[8 + N : 16 + N] = jnp.zeros((8, C), F32)
        for r in range(R):
            pad[8 + r * T : 8 + (r + 1) * T] = rbuf[which, r].astype(F32)
        taps = own_taps[which, :, own_at].astype(F32)
        for r in range(R):
            a = r * T
            made = (
                taps[0:1] * pad[7 + a : 7 + a + T]
                + taps[1:2] * pad[8 + a : 8 + a + T]
                + taps[2:3] * pad[9 + a : 9 + a + T]
            ).astype(BF16).astype(F32)
            xs[a : a + T] = made if which == 0 else made * xs[a : a + T]

    for d in range(1, R):
        in_copy(0, d).wait_recv()

    @pl.when(jnp.logical_not(even))
    def _():
        send(1, 1)
        send(1, 0)

    short(0)
    bias = fb[:, own_at]

    def signal_in(exact):
        def body(step, carry):
            at = step * CHUNK
            blocks = [(xs[rows_at(n1, at), :], None) for n1 in range(L)]
            put_leaves(split_tree(blocks, math.pi / 2), at, exact)
            return carry

        lax.fori_loop(0, steps, body, 0)

    signal_in(EXACT)
    through(0, EXACT)

    def middle(step, carry):
        at = step * CHUNK
        convolved = join_tree(get_leaves(at), math.pi / 2, True)
        for n1 in range(L):
            here = rows_at(n1, at)
            xs[here, :] = convolved[n1] + bias[0:1] * xs[here, :]
        return carry

    lax.fori_loop(0, steps, middle, 0)
    ld_wb.wait()
    gb[...] = dot(tok[...], wb[...]).astype(BF16)
    for side in range(2):
        halo_copy(side).start()
    for d in range(1, R):
        in_copy(1, d).wait_recv()
    short(1)
    signal_in(False)
    through(1, False)

    def last(step, carry):
        at = step * CHUNK
        convolved = join_tree(get_leaves(at), math.pi / 2, True)
        for n1 in range(L):
            value = convolved[n1] + bias[1:2] * xs[rows_at(n1, at), :]
            r, inner = (n1 * LEAF) // T, (n1 * LEAF) % T
            s2[r, pl.ds(pl.multiple_of(inner + at, CHUNK), CHUNK), :] = value.astype(BF16)
        return carry

    for part in range(2):
        lax.fori_loop(part * steps // 2, (part + 1) * steps // 2, last, 0)
        for j in range(R - 1):
            for n1 in range(T // LEAF):
                back_out(j, pl.ds(n1 * LEAF + part * LEAF // 2, LEAF // 2)).start()
    r2[row] = s2[row]

    for side in range(2):
        halo_copy(side).wait_recv()
    before = halo[0, CHUNK - 8 : CHUNK].astype(F32)
    after = halo[1, 0:8].astype(F32)
    gpad[0:8] = jnp.where(row > 0, before, 0.0)
    gpad[8 : 8 + T] = gb[...].astype(F32)
    gpad[8 + T : 16 + T] = jnp.where(row < R - 1, after, 0.0)
    taps = gate_taps[2, :, share_at].astype(F32)
    gbs[...] = (
        taps[0:1] * gpad[7 : 7 + T] + taps[1:2] * gpad[8 : 8 + T] + taps[2:3] * gpad[9 : 9 + T]
    ).astype(BF16).astype(F32)
    for d in range(1, R):
        back_in(d).wait_recv()
    for r in range(R):
        lanes = slice(r * C, (r + 1) * C)
        out_ref[:, lanes] = (gbs[:, lanes] * r2[r].astype(F32)).astype(BF16)
    for d in range(1, R):
        for which in range(2):
            in_copy(which, d).wait_send()
        back_in(d).wait_send()
    for side in range(2):
        halo_copy(side).wait_send()


def per_device(
    tokens, w_value, w_gate_a, w_gate_b, short_taps, pos_weight, pos_bias, sine_freq,
    hid_weight, hid_bias, filter_out, filter_bias, lag_decay,
):
    R = lax.axis_size("row")
    T, D = tokens.shape
    N = T * R
    S = w_value.shape[1]
    C = S // R
    PE, HID = pos_weight.shape
    L = N // LEAF
    row, col = lax.axis_index("row"), lax.axis_index("col")
    fcat, gcat, twist, feat = tables(N, C, PE, HID)
    own_w = filter_out
    own_taps, gate_taps, fb, ld = short_taps, short_taps, filter_bias, lag_decay[None]
    if C % 128:
        own_w = lax.dynamic_slice_in_dim(own_w, row * C, C, 3)
        start = col * S + row * C
        own_taps = lax.dynamic_slice_in_dim(own_taps, start, C, 2)
        gate_taps = lax.dynamic_slice_in_dim(gate_taps, col * S, S, 2)
        fb = lax.dynamic_slice_in_dim(fb, start, C, 1)
        ld = lax.dynamic_slice_in_dim(ld, start, C, 1)
    vm = pl.BlockSpec(memory_space=pltpu.VMEM)
    hbm = pl.BlockSpec(memory_space=pl.ANY)
    dma = pltpu.SemaphoreType.DMA
    small = [own_taps, gate_taps, pos_weight, pos_bias[None], sine_freq, hid_weight, hid_bias[None], fb, ld]
    return pl.pallas_call(
        functools.partial(kernel, (R, T, N, C, S, HID, PE)),
        out_shape=jax.ShapeDtypeStruct((T, S), BF16),
        in_specs=[hbm] * 18,
        out_specs=vm,
        scratch_shapes=[pltpu.VMEM(x.shape, x.dtype) for x in small] + [
            pltpu.VMEM((T, D), BF16),
            pltpu.VMEM((T, S // 2), F32),
            pltpu.VMEM((2, D, S), BF16),
            pltpu.VMEM((D, S), BF16),
            pltpu.VMEM(fcat.shape, BF16),
            pltpu.VMEM(gcat.shape, BF16),
            pltpu.VMEM(twist.shape, F32),
            pltpu.VMEM(feat.shape, BF16),
            pltpu.VMEM((HID, 2, 2, C), F32),
            pltpu.VMEM((2, R, T, C), BF16),
            pltpu.VMEM((2, R, T, C), BF16),
            pltpu.VMEM((T, S), BF16),
            pltpu.VMEM((2, CHUNK, S), BF16),
            pltpu.VMEM((N + 16, C), F32),
            pltpu.VMEM((N, C), F32),
            pltpu.VMEM((T + 16, S), F32),
            pltpu.VMEM((T, S), F32),
            pltpu.VMEM((2 * HID, 2 * HID), F32),
            pltpu.VMEM((2 * HID, 2 * HID), F32),
            pltpu.VMEM((4 * HID, 4 * HID), BF16),
            pltpu.VMEM((4 * HID, 4 * HID), BF16),
            pltpu.VMEM((2, 4 * HID, 2 * C), BF16),
            pltpu.VMEM((2, N, C), F32),
            pltpu.VMEM((2, N, C), F32),
            pltpu.VMEM((2 * LEAF, L * C), BF16),
            pltpu.VMEM((2 * LEAF, L * C), BF16),
            pltpu.VMEM((2, 2 * LEAF, L * C), F32),
            pltpu.VMEM((2 * LEAF, L * C), F32),
            pltpu.VMEM((R, T, C), BF16),
            pltpu.VMEM((R, T, C), BF16),
            dma((22,)),
            dma((2, R)),
            dma((2, R)),
            dma((2,)),
            dma((2,)),
            dma((R,)),
            dma((R,)),
        ],
        compiler_params=pltpu.CompilerParams(
            collective_id=0, has_side_effects=True, vmem_limit_bytes=44 * 1024 * 1024
        ),
    )(*[
        pltpu.with_memory_space_constraint(jnp.asarray(x), pltpu.HBM)
        for x in (tokens, w_value, w_gate_a, w_gate_b, fcat, gcat, twist, feat, own_w, *small)
    ])


def solution(mesh):
    in_specs = (
        P(("grp", "row"), None), P(None, "col"), P(None, "col"), P(None, "col"),
        P(), P(), P(), P(), P(), P(), P(None, None, None, "col"), P(), P(),
    )
    return jax.shard_map(
        per_device, mesh=mesh, in_specs=in_specs, out_specs=P(("grp", "row"), "col"), check_vma=False
    )
```

```python
import functools
import math

import jax
import jax.numpy as jnp
import numpy as np
from jax import lax
from jax.experimental import pallas as pl
from jax.experimental.pallas import tpu as pltpu
from jax.sharding import PartitionSpec as P

WINDOW_SHIFT = 0.05
LEAF = 128
CHUNK = 16
PIECE = 256
EXACT = False
MESH = pl.DeviceIdType.MESH
F32 = jnp.float32
BF16 = jnp.bfloat16


def leaf_angles(theta, count):
    if count == 1:
        return [theta]
    half = theta / 2
    return leaf_angles(half, count // 2) + leaf_angles(half + math.pi, count // 2)


def split_np(values):
    high = values.astype(jnp.bfloat16)
    low = (values - high.astype(np.float64)).astype(jnp.bfloat16)
    return high, low


@functools.lru_cache(maxsize=None)
def tables(seq, lanes, features, hidden):
    k = np.arange(LEAF)
    angle = 2 * np.pi / LEAF * ((k[:, None] * k[None, :]) % LEAF)
    cos, sin = np.cos(angle), np.sin(angle)
    forward = np.block([[cos, -sin], [sin, cos]])
    inverse = np.block([[cos, sin], [-sin, cos]]) / seq
    fcat = np.concatenate(split_np(forward), axis=0)
    gcat = np.concatenate(split_np(inverse), axis=0)
    thetas = np.array(leaf_angles(math.pi / 2, seq // LEAF))
    twist = (thetas[:, None] * k[None, :] / LEAF).reshape(-1)
    twist = np.stack([np.cos(twist), np.sin(twist)]).astype(np.float32)
    twist = np.ascontiguousarray(np.broadcast_to(twist[:, :, None], (2, seq, lanes)))
    bands = (features - 1) // 2
    freq = np.linspace(0.0001, bands - 1, bands, dtype=np.float32)

    def feats(positions):
        positions = positions.astype(np.float32)
        scaled = positions / np.float32(max(seq - 1, 1))
        ang = (np.float32(2.0 * math.pi / seq) * positions)[:, None] * freq[None, :]
        ang = ang.astype(np.float64)
        return np.concatenate([scaled[:, None], np.cos(ang), -np.sin(ang)], axis=1)

    both = np.zeros((seq, 2 * hidden))
    both[:, :features] = feats(np.arange(seq))
    both[:, hidden : hidden + features] = feats(seq - np.arange(seq))
    feat = np.concatenate(split_np(both), axis=1)
    return fcat, gcat, twist, feat


def split(x):
    high = x.astype(BF16)
    return high, (x - high.astype(F32)).astype(BF16)


def dot(a, b):
    return jnp.dot(a, b, preferred_element_type=F32)


def deep(acc, a, b, add=False):
    half = b.shape[0] // 2
    for i, part in enumerate((slice(0, half), slice(half, None))):
        made = dot(a[:, part], b[part])
        acc[i] = acc[i] + made if add else made


PI_A = 3.140625
PI_B = float(np.float32(math.pi - 3.140625))
PI_C = float(math.pi - 3.140625 - np.float32(math.pi - 3.140625))


def sine(x):
    k = jnp.floor(x * (1.0 / math.pi) + 0.5)
    r = x - k * PI_A
    r = r - k * PI_B
    r = r - k * PI_C
    parity = k - 2.0 * jnp.floor(k * 0.5)
    s = r * r
    p = -1.0 / 39916800.0
    for c in (1.0 / 362880.0, -1.0 / 5040.0, 1.0 / 120.0, -1.0 / 6.0):
        p = p * s + c
    return (r + r * s * p) * (1.0 - 2.0 * parity)


def split_tree(blocks, theta):
    if len(blocks) == 1:
        return blocks
    half = len(blocks) // 2
    wr, wi = math.cos(theta / 2), math.sin(theta / 2)
    up, down = [], []
    for (ar, ai), (br, bi) in zip(blocks[:half], blocks[half:]):
        if bi is None:
            tr, ti = br * wr, br * wi
            up.append((ar + tr, ti))
            down.append((ar - tr, -ti))
        else:
            tr, ti = br * wr - bi * wi, br * wi + bi * wr
            up.append((ar + tr, ai + ti))
            down.append((ar - tr, ai - ti))
    return split_tree(up, theta / 2) + split_tree(down, theta / 2 + math.pi)


def join_tree(leaves, theta, top):
    if len(leaves) == 1:
        return leaves
    half = len(leaves) // 2
    up = join_tree(leaves[:half], theta / 2, False)
    down = join_tree(leaves[half:], theta / 2 + math.pi, False)
    wr, wi = math.cos(theta / 2), math.sin(theta / 2)
    first, second = [], []
    for (pr, pi), (qr, qi) in zip(up, down):
        dr, di = pr - qr, pi - qi
        if top:
            first.append(pr + qr)
            second.append(dr * wr + di * wi)
        else:
            first.append((pr + qr, pi + qi))
            second.append((dr * wr + di * wi, di * wr - dr * wi))
    return first + second


def kernel(
    sizes,
    tok_h, wv_h, wa_h, wb_h, fcat_h, gcat_h, twist_h, feat_h,
    wf_h, own_taps_h, gate_taps_h, pw_h, pb_h, sf_h, hw_h, hb_h, fb_h, ld_h,
    out_ref,
    own_taps, gate_taps, pw, pb, sf, hw, hb, fb, ld,
    tok, acc, wva, wb, fcat, gcat, twist, feat,
    wf, sbuf, rbuf, gb, halo, pad, xs, gpad, gbs,
    pwb, hwb, w1, w2, w3, kre, kim, xhi, xlo, spec, ybuf, s2, r2,
    in_sem, send_sem, recv_sem, halo_send, halo_recv, back_send, back_recv,
):
    R, T, N, C, S, HID, PE = sizes
    D = tok.shape[1]
    L = N // LEAF
    row = lax.axis_index("row")
    col = lax.axis_index("col")
    aligned = C % 128 == 0
    if aligned:
        own_at = pl.ds(pl.multiple_of(col * S + row * C, 128), C)
        share_at = pl.ds(pl.multiple_of(col * S, 128), S)
    else:
        own_at, share_at = slice(0, C), slice(0, S)

    half = R // 2
    H = S // 2
    low = row < half
    inner = row > 0
    first = lax.rem(row, half)
    far = [jnp.where(low, half + i, half - 1 - i) for i in range(half)]
    near = [jnp.where(low, 0, half) + lax.rem(first + i, half) for i in range(1, half)]
    order = [jnp.where(low, 1, 0), jnp.where(low, 0, 1)]

    def load(i, src, dst):
        copy = pltpu.make_async_copy(src, dst, in_sem.at[i])
        copy.start()
        return copy

    def load_half(i, src, which, k, rows=slice(None)):
        lanes = pl.ds(pl.multiple_of(order[k] * H, H), H)
        return load(i, src.at[rows, lanes], wva.at[k, rows, which * H : (which + 1) * H])

    halves = [slice(0, D // 2), slice(D // 2, D)]
    ld_first = []
    for i, part in enumerate(halves):
        ld_first.append([
            load(2 * i, tok_h.at[:, part], tok.at[:, part]),
            load_half(2 * i + 1, wv_h, 0, 0, part),
        ])

    barrier = pltpu.get_barrier_semaphore()
    peers = [lax.rem(row + d, R) for d in range(R)]
    sources = [lax.rem(row + R - d, R) for d in range(R)]
    for d in range(1, R):
        pl.semaphore_signal(barrier, inc=1, device_id={"row": peers[d]}, device_id_type=MESH)

    def pieces(total, size):
        return [pl.ds(at, size) for at in range(0, total, size)]

    def out_copy(which, target, slot, part):
        return pltpu.make_async_remote_copy(
            src_ref=sbuf.at[which, target, part], dst_ref=rbuf.at[which, row, part],
            send_sem=send_sem.at[which, slot], recv_sem=recv_sem.at[which, row],
            device_id={"row": target}, device_id_type=MESH)

    def in_copy(which, d):
        return pltpu.make_async_remote_copy(
            src_ref=sbuf.at[which, peers[d]], dst_ref=rbuf.at[which, sources[d]],
            send_sem=send_sem.at[which, d - 1], recv_sem=recv_sem.at[which, sources[d]],
            device_id={"row": peers[d]}, device_id_type=MESH)

    def halo_copy(side):
        src = gb.at[pl.ds(T - CHUNK, CHUNK)] if side == 0 else gb.at[pl.ds(0, CHUNK)]
        target = peers[1] if side == 0 else peers[R - 1]
        return pltpu.make_async_remote_copy(
            src_ref=src, dst_ref=halo.at[side],
            send_sem=halo_send.at[side], recv_sem=halo_recv.at[side],
            device_id={"row": target}, device_id_type=MESH)

    def back_out(j):
        target = (far[::-1] + near)[j]
        return pltpu.make_async_remote_copy(
            src_ref=s2.at[target], dst_ref=r2.at[row],
            send_sem=back_send.at[j], recv_sem=back_recv.at[row],
            device_id={"row": target}, device_id_type=MESH)

    def back_in(d):
        return pltpu.make_async_remote_copy(
            src_ref=s2.at[peers[d]], dst_ref=r2.at[sources[d]],
            send_sem=back_send.at[d - 1], recv_sem=back_recv.at[sources[d]],
            device_id={"row": peers[d]}, device_id_type=MESH)

    def send(which, k):
        for slot, target in enumerate(near if k else far):
            for part in pieces(T, min(PIECE, T)):
                out_copy(which, target, slot + (half if k else 0), part).start()

    def keep(which, k, made):
        for i in range(half):
            sbuf[which, order[k] * half + i] = made[:, i * C : (i + 1) * C]

    for copy in ld_first[0]:
        copy.wait()
    ld_near = [load_half(5 + which, src, which, 1) for which, src in enumerate((wv_h, wa_h))]
    ld_far_a = load_half(4, wa_h, 1, 0)
    small = [
        load(12 + i, src, dst)
        for i, (src, dst) in enumerate([
            (own_taps_h, own_taps), (gate_taps_h, gate_taps), (pw_h, pw), (pb_h, pb),
            (sf_h, sf), (hw_h, hw), (hb_h, hb), (fb_h, fb), (ld_h, ld)])
    ]
    if aligned:
        wf_src = wf_h.at[:, :, :, pl.ds(pl.multiple_of(row * C, 128), C)]
    else:
        wf_src = wf_h
    ld_wf = load(8, wf_src, wf)
    ld_wb = load(7, wb_h, wb)
    ld_feat = load(21, feat_h, feat)
    deep(acc, tok[:, halves[0]], wva[0, halves[0], 0:H])
    for copy in ld_first[1]:
        copy.wait()
    deep(acc, tok[:, halves[1]], wva[0, halves[1], 0:H], True)
    keep(0, 0, (acc[0] + acc[1]).astype(BF16))

    @pl.when(inner)
    def _():
        pl.semaphore_wait(barrier, R - 1)
        send(0, 0)

    for copy in ld_near:
        copy.wait()
    made = dot(tok[...], wva[1]).astype(BF16)
    keep(0, 1, made[:, 0:H])
    keep(1, 1, made[:, H : 2 * H])

    @pl.when(jnp.logical_not(inner))
    def _():
        pl.semaphore_wait(barrier, R - 1)
        send(0, 1)
        send(0, 0)

    ld_far_a.wait()
    deep(acc, tok[...], wva[0, :, H : 2 * H])
    keep(1, 0, (acc[0] + acc[1]).astype(BF16))

    @pl.when(inner)
    def _():
        send(0, 1)

    even = lax.rem(col, 2) == 0
    @pl.when(even)
    def _():
        send(1, 1)
        send(1, 0)

    for which in range(2):
        rbuf[which, row] = sbuf[which, row]
    ld_fcat, ld_twist, ld_gcat = load(9, fcat_h, fcat), load(10, twist_h, twist), load(11, gcat_h, gcat)
    for copy in small:
        copy.wait()
    W = 2 * HID
    pwb[...] = jnp.zeros_like(pwb)
    pwb[0:PE, 0:HID] = pw[...]
    pwb[HID : HID + PE, HID : 2 * HID] = pw[...]
    hwb[...] = jnp.zeros_like(hwb)
    hwb[0:HID, 0:HID] = hw[...]
    hwb[HID : 2 * HID, HID : 2 * HID] = hw[...]
    for w, full in ((w1, pwb), (w2, hwb)):
        high, low = split(full[...])
        w[0:W, 0:W] = high
        w[0:W, W : 2 * W] = low
        w[W : 2 * W, 0:W] = high
        w[W : 2 * W, W : 2 * W] = jnp.zeros_like(low)
    ld_wf.wait()
    for o in range(2):
        for way in range(2):
            high, low = split(wf[:, o, way, :])
            for at, part in enumerate((high, high, low, low)):
                w3[way, at * HID : (at + 1) * HID, o * C : (o + 1) * C] = part
    ld_feat.wait()

    def twice(v):
        return jnp.concatenate([v, v], axis=-1)

    decay = ld[:, own_at]
    rows_f = 256
    pb2, hb2, sf2 = twice(pb[...]), twice(hb[...]), twice(sf[...])

    def filter_rows(step, carry):
        at = pl.ds(pl.multiple_of(step * rows_f, rows_f), rows_f)
        both = dot(feat[at, :], w1[...])
        ha = sine(sf2[0:1] * (both[:, 0:W] + both[:, W : 2 * W] + pb2))
        both = dot(jnp.concatenate(split(ha), axis=-1), w2[...])
        hb_ = sine(sf2[1:2] * (both[:, 0:W] + both[:, W : 2 * W] + hb2))
        swapped = pltpu.roll(hb_, HID, 1)
        lower = lax.broadcasted_iota(jnp.int32, (rows_f, W), 1) < HID
        raw = []
        for way, (head, tail) in enumerate(((hb_, swapped), (swapped, hb_))):
            part = jnp.where(lower, head, tail - tail.astype(BF16).astype(F32)).astype(BF16)
            raw.append(dot(jnp.concatenate([part, part], axis=-1), w3[way]))
        index = (lax.broadcasted_iota(jnp.int32, (rows_f, C), 0) + step * rows_f).astype(F32)
        scale = 1.0 / max(N - 1, 1)
        env_f = jnp.exp(-(index * scale) * decay) + WINDOW_SHIFT
        env_b = jnp.exp(-((N - index) * scale) * decay) + WINDOW_SHIFT
        env_b = jnp.where(index > 0.0, -env_b, 0.0)
        for o in range(2):
            kre[o, at, :] = raw[0][:, o * C : (o + 1) * C] * env_f
            kim[o, at, :] = raw[1][:, o * C : (o + 1) * C] * env_b
        return carry

    lax.fori_loop(0, N // rows_f, filter_rows, 0, unroll=2)
    ld_fcat.wait()
    ld_twist.wait()
    ld_gcat.wait()

    def put_leaves(leaves, at, exact):
        for j, (re, im) in enumerate(leaves):
            tat = pl.ds(pl.multiple_of(j * LEAF + at, CHUNK), CHUNK)
            tc, ts = twist[0, tat, :], twist[1, tat, :]
            zr, zi = re * tc - im * ts, re * ts + im * tc
            lanes = slice(j * C, (j + 1) * C)
            for part, base in ((zr, 0), (zi, LEAF)):
                pat = pl.ds(pl.multiple_of(base + at, CHUNK), CHUNK)
                if exact:
                    xhi[pat, lanes], xlo[pat, lanes] = split(part)
                else:
                    xhi[pat, lanes] = part.astype(BF16)

    def get_leaves(at):
        leaves = []
        for j in range(L):
            tat = pl.ds(pl.multiple_of(j * LEAF + at, CHUNK), CHUNK)
            tc, ts = twist[0, tat, :], twist[1, tat, :]
            lanes = slice(j * C, (j + 1) * C)
            zr = ybuf[pl.ds(pl.multiple_of(at, CHUNK), CHUNK), lanes]
            zi = ybuf[pl.ds(pl.multiple_of(LEAF + at, CHUNK), CHUNK), lanes]
            leaves.append((zr * tc + zi * ts, zi * tc - zr * ts))
        return leaves

    width = 256 if (L * C) % 256 == 0 else L * C
    K2 = 2 * LEAF

    def mul3(cat, hi, lo):
        both = dot(cat[...], hi)
        return both[:K2] + both[K2:] + dot(cat[0:K2], lo)

    steps = LEAF // CHUNK

    def rows_at(n1, at):
        return pl.ds(pl.multiple_of(n1 * LEAF + at, CHUNK), CHUNK)

    for o in range(2):
        def kernel_in(step, carry, o=o):
            at = step * CHUNK
            blocks = [(kre[o, rows_at(n1, at), :], kim[o, rows_at(n1, at), :]) for n1 in range(L)]
            put_leaves(split_tree(blocks, math.pi / 2), at, EXACT)
            return carry

        lax.fori_loop(0, steps, kernel_in, 0)
        for tile in range(L * C // width):
            lanes = slice(tile * width, (tile + 1) * width)
            if EXACT:
                spec[o, :, lanes] = mul3(fcat, xhi[:, lanes], xlo[:, lanes])
            else:
                spec[o, :, lanes] = dot(fcat[0:K2], xhi[:, lanes])

    def through(o, exact):
        for tile in range(L * C // width):
            lanes = slice(tile * width, (tile + 1) * width)
            if exact:
                z = mul3(fcat, xhi[:, lanes], xlo[:, lanes])
            else:
                z = dot(fcat[0:K2], xhi[:, lanes])
            zr, zi = z[:LEAF], z[LEAF:]
            kr, ki = spec[o, 0:LEAF, lanes], spec[o, LEAF:K2, lanes]
            y = jnp.concatenate([zr * kr - zi * ki, zr * ki + zi * kr], axis=0)
            if exact:
                ybuf[:, lanes] = mul3(gcat, *split(y))
            else:
                ybuf[:, lanes] = dot(gcat[0:K2], y.astype(BF16))

    def short(which):
        pad[0:8] = jnp.zeros((8, C), F32)
        pad[8 + N : 16 + N] = jnp.zeros((8, C), F32)
        for r in range(R):
            pad[8 + r * T : 8 + (r + 1) * T] = rbuf[which, r].astype(F32)
        taps = own_taps[which, :, own_at].astype(F32)
        for r in range(R):
            a = r * T
            made = (
                taps[0:1] * pad[7 + a : 7 + a + T]
                + taps[1:2] * pad[8 + a : 8 + a + T]
                + taps[2:3] * pad[9 + a : 9 + a + T]
            ).astype(BF16).astype(F32)
            xs[a : a + T] = made if which == 0 else made * xs[a : a + T]

    for d in range(1, R):
        in_copy(0, d).wait_recv()

    short(0)
    bias = fb[:, own_at]

    def signal_in(exact):
        def body(step, carry):
            at = step * CHUNK
            blocks = [(xs[rows_at(n1, at), :], None) for n1 in range(L)]
            put_leaves(split_tree(blocks, math.pi / 2), at, exact)
            return carry

        lax.fori_loop(0, steps, body, 0)

    signal_in(EXACT)
    through(0, EXACT)

    def middle(step, carry):
        at = step * CHUNK
        convolved = join_tree(get_leaves(at), math.pi / 2, True)
        for n1 in range(L):
            here = rows_at(n1, at)
            xs[here, :] = convolved[n1] + bias[0:1] * xs[here, :]
        return carry

    lax.fori_loop(0, steps, middle, 0)
    @pl.when(jnp.logical_not(even))
    def _():
        send(1, 1)
        send(1, 0)

    ld_wb.wait()
    gb[...] = dot(tok[...], wb[...]).astype(BF16)
    for side in range(2):
        halo_copy(side).start()
    for d in range(1, R):
        in_copy(1, d).wait_recv()
    short(1)
    signal_in(False)
    through(1, False)

    def last(step, carry):
        at = step * CHUNK
        convolved = join_tree(get_leaves(at), math.pi / 2, True)
        for n1 in range(L):
            value = convolved[n1] + bias[1:2] * xs[rows_at(n1, at), :]
            r, inner = (n1 * LEAF) // T, (n1 * LEAF) % T
            s2[r, pl.ds(pl.multiple_of(inner + at, CHUNK), CHUNK), :] = value.astype(BF16)
        return carry

    lax.fori_loop(0, steps, last, 0)
    for j in range(R - 1):
        back_out(j).start()
    r2[row] = s2[row]

    for side in range(2):
        halo_copy(side).wait_recv()
    before = halo[0, CHUNK - 8 : CHUNK].astype(F32)
    after = halo[1, 0:8].astype(F32)
    gpad[0:8] = jnp.where(row > 0, before, 0.0)
    gpad[8 : 8 + T] = gb[...].astype(F32)
    gpad[8 + T : 16 + T] = jnp.where(row < R - 1, after, 0.0)
    taps = gate_taps[2, :, share_at].astype(F32)
    gbs[...] = (
        taps[0:1] * gpad[7 : 7 + T] + taps[1:2] * gpad[8 : 8 + T] + taps[2:3] * gpad[9 : 9 + T]
    ).astype(BF16).astype(F32)
    for d in range(1, R):
        back_in(d).wait_recv()
    for r in range(R):
        lanes = slice(r * C, (r + 1) * C)
        out_ref[:, lanes] = (gbs[:, lanes] * r2[r].astype(F32)).astype(BF16)
    for d in range(1, R):
        for which in range(2):
            in_copy(which, d).wait_send()
        back_in(d).wait_send()
    for side in range(2):
        halo_copy(side).wait_send()


def per_device(
    tokens, w_value, w_gate_a, w_gate_b, short_taps, pos_weight, pos_bias, sine_freq,
    hid_weight, hid_bias, filter_out, filter_bias, lag_decay,
):
    R = lax.axis_size("row")
    T, D = tokens.shape
    N = T * R
    S = w_value.shape[1]
    C = S // R
    PE, HID = pos_weight.shape
    L = N // LEAF
    row, col = lax.axis_index("row"), lax.axis_index("col")
    fcat, gcat, twist, feat = tables(N, C, PE, HID)
    own_w = filter_out
    own_taps, gate_taps, fb, ld = short_taps, short_taps, filter_bias, lag_decay[None]
    if C % 128:
        own_w = lax.dynamic_slice_in_dim(own_w, row * C, C, 3)
        start = col * S + row * C
        own_taps = lax.dynamic_slice_in_dim(own_taps, start, C, 2)
        gate_taps = lax.dynamic_slice_in_dim(gate_taps, col * S, S, 2)
        fb = lax.dynamic_slice_in_dim(fb, start, C, 1)
        ld = lax.dynamic_slice_in_dim(ld, start, C, 1)
    vm = pl.BlockSpec(memory_space=pltpu.VMEM)
    hbm = pl.BlockSpec(memory_space=pl.ANY)
    dma = pltpu.SemaphoreType.DMA
    small = [own_taps, gate_taps, pos_weight, pos_bias[None], sine_freq, hid_weight, hid_bias[None], fb, ld]
    return pl.pallas_call(
        functools.partial(kernel, (R, T, N, C, S, HID, PE)),
        out_shape=jax.ShapeDtypeStruct((T, S), BF16),
        in_specs=[hbm] * 18,
        out_specs=vm,
        scratch_shapes=[pltpu.VMEM(x.shape, x.dtype) for x in small] + [
            pltpu.VMEM((T, D), BF16),
            pltpu.VMEM((2, T, S // 2), F32),
            pltpu.VMEM((2, D, S), BF16),
            pltpu.VMEM((D, S), BF16),
            pltpu.VMEM(fcat.shape, BF16),
            pltpu.VMEM(gcat.shape, BF16),
            pltpu.VMEM(twist.shape, F32),
            pltpu.VMEM(feat.shape, BF16),
            pltpu.VMEM((HID, 2, 2, C), F32),
            pltpu.VMEM((2, R, T, C), BF16),
            pltpu.VMEM((2, R, T, C), BF16),
            pltpu.VMEM((T, S), BF16),
            pltpu.VMEM((2, CHUNK, S), BF16),
            pltpu.VMEM((N + 16, C), F32),
            pltpu.VMEM((N, C), F32),
            pltpu.VMEM((T + 16, S), F32),
            pltpu.VMEM((T, S), F32),
            pltpu.VMEM((2 * HID, 2 * HID), F32),
            pltpu.VMEM((2 * HID, 2 * HID), F32),
            pltpu.VMEM((4 * HID, 4 * HID), BF16),
            pltpu.VMEM((4 * HID, 4 * HID), BF16),
            pltpu.VMEM((2, 4 * HID, 2 * C), BF16),
            pltpu.VMEM((2, N, C), F32),
            pltpu.VMEM((2, N, C), F32),
            pltpu.VMEM((2 * LEAF, L * C), BF16),
            pltpu.VMEM((2 * LEAF, L * C), BF16),
            pltpu.VMEM((2, 2 * LEAF, L * C), F32),
            pltpu.VMEM((2 * LEAF, L * C), F32),
            pltpu.VMEM((R, T, C), BF16),
            pltpu.VMEM((R, T, C), BF16),
            dma((22,)),
            dma((2, R)),
            dma((2, R)),
            dma((2,)),
            dma((2,)),
            dma((R,)),
            dma((R,)),
        ],
        compiler_params=pltpu.CompilerParams(
            collective_id=0, has_side_effects=True, vmem_limit_bytes=44 * 1024 * 1024
        ),
    )(*[
        pltpu.with_memory_space_constraint(jnp.asarray(x), pltpu.HBM)
        for x in (tokens, w_value, w_gate_a, w_gate_b, fcat, gcat, twist, feat, own_w, *small)
    ])


def solution(mesh):
    in_specs = (
        P(("grp", "row"), None), P(None, "col"), P(None, "col"), P(None, "col"),
        P(), P(), P(), P(), P(), P(), P(None, None, None, "col"), P(), P(),
    )
    return jax.shard_map(
        per_device, mesh=mesh, in_specs=in_specs, out_specs=P(("grp", "row"), "col"), check_vma=False
    )
```

```python
import functools
import math

import jax
import jax.numpy as jnp
import numpy as np
from jax import lax
from jax.experimental import pallas as pl
from jax.experimental.pallas import tpu as pltpu
from jax.sharding import PartitionSpec as P

WINDOW_SHIFT = 0.05
LEAF = 128
CHUNK = 16
PIECE = 256
EXACT = False
MESH = pl.DeviceIdType.MESH
F32 = jnp.float32
BF16 = jnp.bfloat16


def leaf_angles(theta, count):
    if count == 1:
        return [theta]
    half = theta / 2
    return leaf_angles(half, count // 2) + leaf_angles(half + math.pi, count // 2)


def split_np(values):
    high = values.astype(jnp.bfloat16)
    low = (values - high.astype(np.float64)).astype(jnp.bfloat16)
    return high, low


@functools.lru_cache(maxsize=None)
def tables(seq, lanes, features, hidden):
    k = np.arange(LEAF)
    angle = 2 * np.pi / LEAF * ((k[:, None] * k[None, :]) % LEAF)
    cos, sin = np.cos(angle), np.sin(angle)
    forward = np.block([[cos, -sin], [sin, cos]])
    inverse = np.block([[cos, sin], [-sin, cos]]) / seq
    fcat = np.concatenate(split_np(forward), axis=0)
    gcat = np.concatenate(split_np(inverse), axis=0)
    thetas = np.array(leaf_angles(math.pi / 2, seq // LEAF))
    twist = (thetas[:, None] * k[None, :] / LEAF).reshape(-1)
    twist = np.stack([np.cos(twist), np.sin(twist)]).astype(np.float32)
    twist = np.ascontiguousarray(np.broadcast_to(twist[:, :, None], (2, seq, lanes)))
    bands = (features - 1) // 2
    freq = np.linspace(0.0001, bands - 1, bands, dtype=np.float32)

    def feats(positions):
        positions = positions.astype(np.float32)
        scaled = positions / np.float32(max(seq - 1, 1))
        ang = (np.float32(2.0 * math.pi / seq) * positions)[:, None] * freq[None, :]
        ang = ang.astype(np.float64)
        return np.concatenate([scaled[:, None], np.cos(ang), -np.sin(ang)], axis=1)

    both = np.zeros((seq, 2 * hidden))
    both[:, :features] = feats(np.arange(seq))
    both[:, hidden : hidden + features] = feats(seq - np.arange(seq))
    feat = np.concatenate(split_np(both), axis=1)
    return fcat, gcat, twist, feat


def split(x):
    high = x.astype(BF16)
    return high, (x - high.astype(F32)).astype(BF16)


def dot(a, b):
    return jnp.dot(a, b, preferred_element_type=F32)


def deep(acc, a, b, add=False):
    half = b.shape[0] // 2
    for i, part in enumerate((slice(0, half), slice(half, None))):
        made = dot(a[:, part], b[part])
        acc[i] = acc[i] + made if add else made


PI_A = 3.140625
PI_B = float(np.float32(math.pi - 3.140625))
PI_C = float(math.pi - 3.140625 - np.float32(math.pi - 3.140625))


def sine(x):
    k = jnp.floor(x * (1.0 / math.pi) + 0.5)
    r = x - k * PI_A
    r = r - k * PI_B
    r = r - k * PI_C
    parity = k - 2.0 * jnp.floor(k * 0.5)
    s = r * r
    p = -1.0 / 39916800.0
    for c in (1.0 / 362880.0, -1.0 / 5040.0, 1.0 / 120.0, -1.0 / 6.0):
        p = p * s + c
    return (r + r * s * p) * (1.0 - 2.0 * parity)


def split_tree(blocks, theta):
    if len(blocks) == 1:
        return blocks
    half = len(blocks) // 2
    wr, wi = math.cos(theta / 2), math.sin(theta / 2)
    up, down = [], []
    for (ar, ai), (br, bi) in zip(blocks[:half], blocks[half:]):
        if bi is None:
            tr, ti = br * wr, br * wi
            up.append((ar + tr, ti))
            down.append((ar - tr, -ti))
        else:
            tr, ti = br * wr - bi * wi, br * wi + bi * wr
            up.append((ar + tr, ai + ti))
            down.append((ar - tr, ai - ti))
    return split_tree(up, theta / 2) + split_tree(down, theta / 2 + math.pi)


def join_tree(leaves, theta, top):
    if len(leaves) == 1:
        return leaves
    half = len(leaves) // 2
    up = join_tree(leaves[:half], theta / 2, False)
    down = join_tree(leaves[half:], theta / 2 + math.pi, False)
    wr, wi = math.cos(theta / 2), math.sin(theta / 2)
    first, second = [], []
    for (pr, pi), (qr, qi) in zip(up, down):
        dr, di = pr - qr, pi - qi
        if top:
            first.append(pr + qr)
            second.append(dr * wr + di * wi)
        else:
            first.append((pr + qr, pi + qi))
            second.append((dr * wr + di * wi, di * wr - dr * wi))
    return first + second


def kernel(
    sizes,
    tok_h, wv_h, wa_h, wb_h, fcat_h, gcat_h, twist_h, feat_h,
    wf_h, own_taps_h, gate_taps_h, pw_h, pb_h, sf_h, hw_h, hb_h, fb_h, ld_h,
    out_ref,
    own_taps, gate_taps, pw, pb, sf, hw, hb, fb, ld,
    tok, acc, wva, wb, fcat, gcat, twist, feat,
    wf, sbuf, rbuf, gb, halo, pad, xs, gpad, gbs,
    pwb, hwb, w1, w2, w3, kre, kim, xhi, xlo, spec, ybuf, s2, r2,
    in_sem, send_sem, recv_sem, halo_send, halo_recv, back_send, back_recv,
):
    R, T, N, C, S, HID, PE = sizes
    D = tok.shape[1]
    L = N // LEAF
    row = lax.axis_index("row")
    col = lax.axis_index("col")
    aligned = C % 128 == 0
    if aligned:
        own_at = pl.ds(pl.multiple_of(col * S + row * C, 128), C)
        share_at = pl.ds(pl.multiple_of(col * S, 128), S)
    else:
        own_at, share_at = slice(0, C), slice(0, S)

    half = R // 2
    H = S // 2
    low = row < half
    inner = row > 0
    first = lax.rem(row, half)
    far = [jnp.where(low, half + i, half - 1 - i) for i in range(half)]
    near = [jnp.where(low, 0, half) + lax.rem(first + i, half) for i in range(1, half)]
    order = [jnp.where(low, 1, 0), jnp.where(low, 0, 1)]

    def load(i, src, dst):
        copy = pltpu.make_async_copy(src, dst, in_sem.at[i])
        copy.start()
        return copy

    def load_half(i, src, which, k, rows=slice(None)):
        lanes = pl.ds(pl.multiple_of(order[k] * H, H), H)
        return load(i, src.at[rows, lanes], wva.at[k, rows, which * H : (which + 1) * H])

    halves = [slice(0, D // 2), slice(D // 2, D)]
    ld_first = []
    for i, part in enumerate(halves):
        ld_first.append([
            load(2 * i, tok_h.at[:, part], tok.at[:, part]),
            load_half(2 * i + 1, wv_h, 0, 0, part),
        ])

    barrier = pltpu.get_barrier_semaphore()
    peers = [lax.rem(row + d, R) for d in range(R)]
    sources = [lax.rem(row + R - d, R) for d in range(R)]
    for d in range(1, R):
        pl.semaphore_signal(barrier, inc=1, device_id={"row": peers[d]}, device_id_type=MESH)

    def pieces(total, size):
        return [pl.ds(at, size) for at in range(0, total, size)]

    def out_copy(which, target, slot, part):
        return pltpu.make_async_remote_copy(
            src_ref=sbuf.at[which, target, part], dst_ref=rbuf.at[which, row, part],
            send_sem=send_sem.at[which, slot], recv_sem=recv_sem.at[which, row],
            device_id={"row": target}, device_id_type=MESH)

    def in_copy(which, d):
        return pltpu.make_async_remote_copy(
            src_ref=sbuf.at[which, peers[d]], dst_ref=rbuf.at[which, sources[d]],
            send_sem=send_sem.at[which, d - 1], recv_sem=recv_sem.at[which, sources[d]],
            device_id={"row": peers[d]}, device_id_type=MESH)

    def halo_copy(side):
        src = gb.at[pl.ds(T - CHUNK, CHUNK)] if side == 0 else gb.at[pl.ds(0, CHUNK)]
        target = peers[1] if side == 0 else peers[R - 1]
        return pltpu.make_async_remote_copy(
            src_ref=src, dst_ref=halo.at[side],
            send_sem=halo_send.at[side], recv_sem=halo_recv.at[side],
            device_id={"row": target}, device_id_type=MESH)

    def back_out(j):
        target = jnp.where(row == 0, (near + far[::-1])[j], (far[::-1] + near)[j])
        return pltpu.make_async_remote_copy(
            src_ref=s2.at[target], dst_ref=r2.at[row],
            send_sem=back_send.at[j], recv_sem=back_recv.at[row],
            device_id={"row": target}, device_id_type=MESH)

    def back_in(d):
        return pltpu.make_async_remote_copy(
            src_ref=s2.at[peers[d]], dst_ref=r2.at[sources[d]],
            send_sem=back_send.at[d - 1], recv_sem=back_recv.at[sources[d]],
            device_id={"row": peers[d]}, device_id_type=MESH)

    def send(which, k):
        for slot, target in enumerate(near if k else far):
            for part in pieces(T, min(PIECE, T)):
                out_copy(which, target, slot + (half if k else 0), part).start()

    def keep(which, k, made):
        for i in range(half):
            sbuf[which, order[k] * half + i] = made[:, i * C : (i + 1) * C]

    for copy in ld_first[0]:
        copy.wait()
    ld_near = [load_half(5 + which, src, which, 1) for which, src in enumerate((wv_h, wa_h))]
    ld_far_a = load_half(4, wa_h, 1, 0)
    small = [
        load(12 + i, src, dst)
        for i, (src, dst) in enumerate([
            (own_taps_h, own_taps), (gate_taps_h, gate_taps), (pw_h, pw), (pb_h, pb),
            (sf_h, sf), (hw_h, hw), (hb_h, hb), (fb_h, fb), (ld_h, ld)])
    ]
    if aligned:
        wf_src = wf_h.at[:, :, :, pl.ds(pl.multiple_of(row * C, 128), C)]
    else:
        wf_src = wf_h
    ld_wf = load(8, wf_src, wf)
    ld_wb = load(7, wb_h, wb)
    ld_feat = load(21, feat_h, feat)
    deep(acc, tok[:, halves[0]], wva[0, halves[0], 0:H])
    for copy in ld_first[1]:
        copy.wait()
    deep(acc, tok[:, halves[1]], wva[0, halves[1], 0:H], True)
    keep(0, 0, (acc[0] + acc[1]).astype(BF16))

    @pl.when(inner)
    def _():
        pl.semaphore_wait(barrier, R - 1)
        send(0, 0)

    for copy in ld_near:
        copy.wait()
    made = dot(tok[...], wva[1]).astype(BF16)
    keep(0, 1, made[:, 0:H])
    keep(1, 1, made[:, H : 2 * H])

    @pl.when(jnp.logical_not(inner))
    def _():
        pl.semaphore_wait(barrier, R - 1)
        send(0, 1)
        send(0, 0)

    ld_far_a.wait()
    deep(acc, tok[...], wva[0, :, H : 2 * H])
    keep(1, 0, (acc[0] + acc[1]).astype(BF16))

    @pl.when(inner)
    def _():
        send(0, 1)

    even = lax.rem(col, 2) == 0
    @pl.when(even)
    def _():
        send(1, 1)
        send(1, 0)

    for which in range(2):
        rbuf[which, row] = sbuf[which, row]
    ld_fcat, ld_twist, ld_gcat = load(9, fcat_h, fcat), load(10, twist_h, twist), load(11, gcat_h, gcat)
    for copy in small:
        copy.wait()
    W = 2 * HID
    pwb[...] = jnp.zeros_like(pwb)
    pwb[0:PE, 0:HID] = pw[...]
    pwb[HID : HID + PE, HID : 2 * HID] = pw[...]
    hwb[...] = jnp.zeros_like(hwb)
    hwb[0:HID, 0:HID] = hw[...]
    hwb[HID : 2 * HID, HID : 2 * HID] = hw[...]
    for w, full in ((w1, pwb), (w2, hwb)):
        high, low = split(full[...])
        w[0:W, 0:W] = high
        w[0:W, W : 2 * W] = low
        w[W : 2 * W, 0:W] = high
        w[W : 2 * W, W : 2 * W] = jnp.zeros_like(low)
    ld_wf.wait()
    for o in range(2):
        for way in range(2):
            high, low = split(wf[:, o, way, :])
            for at, part in enumerate((high, high, low, low)):
                w3[way, at * HID : (at + 1) * HID, o * C : (o + 1) * C] = part
    ld_feat.wait()

    def twice(v):
        return jnp.concatenate([v, v], axis=-1)

    decay = ld[:, own_at]
    rows_f = 256
    pb2, hb2, sf2 = twice(pb[...]), twice(hb[...]), twice(sf[...])

    def filter_rows(step, carry):
        at = pl.ds(pl.multiple_of(step * rows_f, rows_f), rows_f)
        both = dot(feat[at, :], w1[...])
        ha = sine(sf2[0:1] * (both[:, 0:W] + both[:, W : 2 * W] + pb2))
        both = dot(jnp.concatenate(split(ha), axis=-1), w2[...])
        hb_ = sine(sf2[1:2] * (both[:, 0:W] + both[:, W : 2 * W] + hb2))
        swapped = pltpu.roll(hb_, HID, 1)
        lower = lax.broadcasted_iota(jnp.int32, (rows_f, W), 1) < HID
        raw = []
        for way, (head, tail) in enumerate(((hb_, swapped), (swapped, hb_))):
            part = jnp.where(lower, head, tail - tail.astype(BF16).astype(F32)).astype(BF16)
            raw.append(dot(jnp.concatenate([part, part], axis=-1), w3[way]))
        index = (lax.broadcasted_iota(jnp.int32, (rows_f, C), 0) + step * rows_f).astype(F32)
        scale = 1.0 / max(N - 1, 1)
        env_f = jnp.exp(-(index * scale) * decay) + WINDOW_SHIFT
        env_b = jnp.exp(-((N - index) * scale) * decay) + WINDOW_SHIFT
        env_b = jnp.where(index > 0.0, -env_b, 0.0)
        for o in range(2):
            kre[o, at, :] = raw[0][:, o * C : (o + 1) * C] * env_f
            kim[o, at, :] = raw[1][:, o * C : (o + 1) * C] * env_b
        return carry

    lax.fori_loop(0, N // rows_f, filter_rows, 0, unroll=2)
    ld_fcat.wait()
    ld_twist.wait()
    ld_gcat.wait()

    def put_leaves(leaves, at, exact):
        for j, (re, im) in enumerate(leaves):
            tat = pl.ds(pl.multiple_of(j * LEAF + at, CHUNK), CHUNK)
            tc, ts = twist[0, tat, :], twist[1, tat, :]
            zr, zi = re * tc - im * ts, re * ts + im * tc
            lanes = slice(j * C, (j + 1) * C)
            for part, base in ((zr, 0), (zi, LEAF)):
                pat = pl.ds(pl.multiple_of(base + at, CHUNK), CHUNK)
                if exact:
                    xhi[pat, lanes], xlo[pat, lanes] = split(part)
                else:
                    xhi[pat, lanes] = part.astype(BF16)

    def get_leaves(at):
        leaves = []
        for j in range(L):
            tat = pl.ds(pl.multiple_of(j * LEAF + at, CHUNK), CHUNK)
            tc, ts = twist[0, tat, :], twist[1, tat, :]
            lanes = slice(j * C, (j + 1) * C)
            zr = ybuf[pl.ds(pl.multiple_of(at, CHUNK), CHUNK), lanes]
            zi = ybuf[pl.ds(pl.multiple_of(LEAF + at, CHUNK), CHUNK), lanes]
            leaves.append((zr * tc + zi * ts, zi * tc - zr * ts))
        return leaves

    width = 256 if (L * C) % 256 == 0 else L * C
    K2 = 2 * LEAF

    def mul3(cat, hi, lo):
        both = dot(cat[...], hi)
        return both[:K2] + both[K2:] + dot(cat[0:K2], lo)

    steps = LEAF // CHUNK

    def rows_at(n1, at):
        return pl.ds(pl.multiple_of(n1 * LEAF + at, CHUNK), CHUNK)

    for o in range(2):
        def kernel_in(step, carry, o=o):
            at = step * CHUNK
            blocks = [(kre[o, rows_at(n1, at), :], kim[o, rows_at(n1, at), :]) for n1 in range(L)]
            put_leaves(split_tree(blocks, math.pi / 2), at, EXACT)
            return carry

        lax.fori_loop(0, steps, kernel_in, 0)
        for tile in range(L * C // width):
            lanes = slice(tile * width, (tile + 1) * width)
            if EXACT:
                spec[o, :, lanes] = mul3(fcat, xhi[:, lanes], xlo[:, lanes])
            else:
                spec[o, :, lanes] = dot(fcat[0:K2], xhi[:, lanes])

    def through(o, exact):
        for tile in range(L * C // width):
            lanes = slice(tile * width, (tile + 1) * width)
            if exact:
                z = mul3(fcat, xhi[:, lanes], xlo[:, lanes])
            else:
                z = dot(fcat[0:K2], xhi[:, lanes])
            zr, zi = z[:LEAF], z[LEAF:]
            kr, ki = spec[o, 0:LEAF, lanes], spec[o, LEAF:K2, lanes]
            y = jnp.concatenate([zr * kr - zi * ki, zr * ki + zi * kr], axis=0)
            if exact:
                ybuf[:, lanes] = mul3(gcat, *split(y))
            else:
                ybuf[:, lanes] = dot(gcat[0:K2], y.astype(BF16))

    def short(which):
        pad[0:8] = jnp.zeros((8, C), F32)
        pad[8 + N : 16 + N] = jnp.zeros((8, C), F32)
        for r in range(R):
            pad[8 + r * T : 8 + (r + 1) * T] = rbuf[which, r].astype(F32)
        taps = own_taps[which, :, own_at].astype(F32)
        for r in range(R):
            a = r * T
            made = (
                taps[0:1] * pad[7 + a : 7 + a + T]
                + taps[1:2] * pad[8 + a : 8 + a + T]
                + taps[2:3] * pad[9 + a : 9 + a + T]
            ).astype(BF16).astype(F32)
            xs[a : a + T] = made if which == 0 else made * xs[a : a + T]

    for d in range(1, R):
        in_copy(0, d).wait_recv()

    short(0)
    bias = fb[:, own_at]

    def signal_in(exact):
        def body(step, carry):
            at = step * CHUNK
            blocks = [(xs[rows_at(n1, at), :], None) for n1 in range(L)]
            put_leaves(split_tree(blocks, math.pi / 2), at, exact)
            return carry

        lax.fori_loop(0, steps, body, 0)

    signal_in(EXACT)
    through(0, EXACT)

    def middle(step, carry):
        at = step * CHUNK
        convolved = join_tree(get_leaves(at), math.pi / 2, True)
        for n1 in range(L):
            here = rows_at(n1, at)
            xs[here, :] = convolved[n1] + bias[0:1] * xs[here, :]
        return carry

    lax.fori_loop(0, steps, middle, 0)
    @pl.when(jnp.logical_not(even))
    def _():
        send(1, 1)
        send(1, 0)

    ld_wb.wait()
    gb[...] = dot(tok[...], wb[...]).astype(BF16)
    for side in range(2):
        halo_copy(side).start()
    for d in range(1, R):
        in_copy(1, d).wait_recv()
    short(1)
    signal_in(False)
    through(1, False)

    def last(step, carry):
        at = step * CHUNK
        convolved = join_tree(get_leaves(at), math.pi / 2, True)
        for n1 in range(L):
            value = convolved[n1] + bias[1:2] * xs[rows_at(n1, at), :]
            r, inner = (n1 * LEAF) // T, (n1 * LEAF) % T
            s2[r, pl.ds(pl.multiple_of(inner + at, CHUNK), CHUNK), :] = value.astype(BF16)
        return carry

    lax.fori_loop(0, steps, last, 0)
    for j in range(R - 1):
        back_out(j).start()
    r2[row] = s2[row]

    for side in range(2):
        halo_copy(side).wait_recv()
    before = halo[0, CHUNK - 8 : CHUNK].astype(F32)
    after = halo[1, 0:8].astype(F32)
    gpad[0:8] = jnp.where(row > 0, before, 0.0)
    gpad[8 : 8 + T] = gb[...].astype(F32)
    gpad[8 + T : 16 + T] = jnp.where(row < R - 1, after, 0.0)
    taps = gate_taps[2, :, share_at].astype(F32)
    gbs[...] = (
        taps[0:1] * gpad[7 : 7 + T] + taps[1:2] * gpad[8 : 8 + T] + taps[2:3] * gpad[9 : 9 + T]
    ).astype(BF16).astype(F32)
    for d in range(1, R):
        back_in(d).wait_recv()
    for r in range(R):
        lanes = slice(r * C, (r + 1) * C)
        out_ref[:, lanes] = (gbs[:, lanes] * r2[r].astype(F32)).astype(BF16)
    for d in range(1, R):
        for which in range(2):
            in_copy(which, d).wait_send()
        back_in(d).wait_send()
    for side in range(2):
        halo_copy(side).wait_send()


def per_device(
    tokens, w_value, w_gate_a, w_gate_b, short_taps, pos_weight, pos_bias, sine_freq,
    hid_weight, hid_bias, filter_out, filter_bias, lag_decay,
):
    R = lax.axis_size("row")
    T, D = tokens.shape
    N = T * R
    S = w_value.shape[1]
    C = S // R
    PE, HID = pos_weight.shape
    L = N // LEAF
    row, col = lax.axis_index("row"), lax.axis_index("col")
    fcat, gcat, twist, feat = tables(N, C, PE, HID)
    own_w = filter_out
    own_taps, gate_taps, fb, ld = short_taps, short_taps, filter_bias, lag_decay[None]
    if C % 128:
        own_w = lax.dynamic_slice_in_dim(own_w, row * C, C, 3)
        start = col * S + row * C
        own_taps = lax.dynamic_slice_in_dim(own_taps, start, C, 2)
        gate_taps = lax.dynamic_slice_in_dim(gate_taps, col * S, S, 2)
        fb = lax.dynamic_slice_in_dim(fb, start, C, 1)
        ld = lax.dynamic_slice_in_dim(ld, start, C, 1)
    vm = pl.BlockSpec(memory_space=pltpu.VMEM)
    hbm = pl.BlockSpec(memory_space=pl.ANY)
    dma = pltpu.SemaphoreType.DMA
    small = [own_taps, gate_taps, pos_weight, pos_bias[None], sine_freq, hid_weight, hid_bias[None], fb, ld]
    return pl.pallas_call(
        functools.partial(kernel, (R, T, N, C, S, HID, PE)),
        out_shape=jax.ShapeDtypeStruct((T, S), BF16),
        in_specs=[hbm] * 18,
        out_specs=vm,
        scratch_shapes=[pltpu.VMEM(x.shape, x.dtype) for x in small] + [
            pltpu.VMEM((T, D), BF16),
            pltpu.VMEM((2, T, S // 2), F32),
            pltpu.VMEM((2, D, S), BF16),
            pltpu.VMEM((D, S), BF16),
            pltpu.VMEM(fcat.shape, BF16),
            pltpu.VMEM(gcat.shape, BF16),
            pltpu.VMEM(twist.shape, F32),
            pltpu.VMEM(feat.shape, BF16),
            pltpu.VMEM((HID, 2, 2, C), F32),
            pltpu.VMEM((2, R, T, C), BF16),
            pltpu.VMEM((2, R, T, C), BF16),
            pltpu.VMEM((T, S), BF16),
            pltpu.VMEM((2, CHUNK, S), BF16),
            pltpu.VMEM((N + 16, C), F32),
            pltpu.VMEM((N, C), F32),
            pltpu.VMEM((T + 16, S), F32),
            pltpu.VMEM((T, S), F32),
            pltpu.VMEM((2 * HID, 2 * HID), F32),
            pltpu.VMEM((2 * HID, 2 * HID), F32),
            pltpu.VMEM((4 * HID, 4 * HID), BF16),
            pltpu.VMEM((4 * HID, 4 * HID), BF16),
            pltpu.VMEM((2, 4 * HID, 2 * C), BF16),
            pltpu.VMEM((2, N, C), F32),
            pltpu.VMEM((2, N, C), F32),
            pltpu.VMEM((2 * LEAF, L * C), BF16),
            pltpu.VMEM((2 * LEAF, L * C), BF16),
            pltpu.VMEM((2, 2 * LEAF, L * C), F32),
            pltpu.VMEM((2 * LEAF, L * C), F32),
            pltpu.VMEM((R, T, C), BF16),
            pltpu.VMEM((R, T, C), BF16),
            dma((22,)),
            dma((2, R)),
            dma((2, R)),
            dma((2,)),
            dma((2,)),
            dma((R,)),
            dma((R,)),
        ],
        compiler_params=pltpu.CompilerParams(
            collective_id=0, has_side_effects=True, vmem_limit_bytes=44 * 1024 * 1024
        ),
    )(*[
        pltpu.with_memory_space_constraint(jnp.asarray(x), pltpu.HBM)
        for x in (tokens, w_value, w_gate_a, w_gate_b, fcat, gcat, twist, feat, own_w, *small)
    ])


def solution(mesh):
    in_specs = (
        P(("grp", "row"), None), P(None, "col"), P(None, "col"), P(None, "col"),
        P(), P(), P(), P(), P(), P(), P(None, None, None, "col"), P(), P(),
    )
    return jax.shard_map(
        per_device, mesh=mesh, in_specs=in_specs, out_specs=P(("grp", "row"), "col"), check_vma=False
    )
```
